32 devices in a mesh: kv: 8 (over z, y), tp: 4 (over x, core).
Axes of the slice: x: 2, y: 2, z: 4, core: 2. Of those that a mesh axis runs over, the one named last changes fastest.
Arguments:
- hidden_vectors: bfloat16 [64, 2048], P(None, 'kv'), may hold values from -24 to 24
- input_norm_gain: float32 [2048], P('kv'), may hold values from 0.1 to 1.9
- gate_matrix: bfloat16 [2048, 4096], P('kv', 'tp'), may hold values from -0.125 to 0.125
- value_matrix: bfloat16 [2048, 4096], P('kv', 'tp'), may hold values from -0.125 to 0.125
- write_matrix: bfloat16 [2048, 2048], P('kv', 'tp'), may hold values from -0.125 to 0.125
- read_matrix: bfloat16 [2048, 2048], P('kv', 'tp'), may hold values from -0.125 to 0.125
- step_matrix: bfloat16 [2048, 64], P('kv', 'tp'), may hold values from -0.125 to 0.125
- raw_value_rows: bfloat16 [16, 7, 4096], P('kv', None, 'tp'), may hold values from -6 to 6
- raw_write_rows: bfloat16 [16, 7, 2048], P('kv', None, 'tp'), may hold values from -6 to 6
- raw_read_rows: bfloat16 [16, 7, 2048], P('kv', None, 'tp'), may hold values from -6 to 6
- value_filter_taps: bfloat16 [4, 4096], P(None, 'tp'), may hold values from -3 to 3
- write_filter_taps: bfloat16 [4, 2048], P(None, 'tp'), may hold values from -3 to 3
- read_filter_taps: bfloat16 [4, 2048], P(None, 'tp'), may hold values from -3 to 3
- step_size_bias: float32 [64], P('tp'), may hold values from -3 to 0
- rate_logarithm: float32 [64], P('tp'), may hold values from -4 to 0.5
- direct_path_gain: float32 [64], P('tp'), may hold values from 0.1 to 1.9
- prior_step_preact: float32 [16, 4, 64], P('kv', None, 'tp'), may hold values from -6 to 6
- extra_log_decay: float32 [16, 8, 64], P('kv', None, 'tp'), may hold values from -0.7 to 0, as said below
- accepted: int32 [16], P('kv'), may hold values from 0 to 4
- prior_state: float32 [16, 64, 64, 128], P('kv', 'tp'), may hold values from -6 to 6
- group_norm_gain: float32 [4096], P('tp'), may hold values from 0.1 to 1.9
- output_matrix: bfloat16 [4096, 2048], P('tp', 'kv'), may hold values from -0.09375 to 0.09375
Outputs:
- mixer_out: bfloat16 [64, 2048], P('tp', 'kv')
- resumed_state: float32 [16, 64, 64, 128], P('kv', 'tp')
The draws below stay inside these ranges and needn't reach their ends.
Inputs may be any that keep to these rules, and one draw needn't show every extreme that they name: `extra_log_decay`: zero at most positions.
All inputs are finite; a program needn't handle non-finite values.
Results may differ from the reference program's by a relative error of at most 0.0095.
Values may be sent and summed in bfloat16 or wider, within the bound.
No kernel may reach another device: no remote copies, remote signals or barrier semaphores. Data moves between devices by JAX's collectives and lax.ppermute only.
A program may use at most 64 MiB of HBM per device.

```python
import math
import jax
import jax.numpy as jnp
from jax import lax

D = 2048
HEADS = 64
HEAD_DIM = 64
GROUPS = 16
STATE = 128
TAPS = 4
DRAFT_TOKENS = 4
INNER = 4096
SEQS = 16
TOKENS = 64
N_TP = 4


def draw_hidden_vectors(key, part):
    normal_base = jax.random.normal(jax.random.fold_in(key, 11), (TOKENS, D), jnp.float32)
    column_scale = jnp.exp(jnp.arange(D, dtype=jnp.float32) * (math.log(4.0) / D)) * 0.5
    values = normal_base * column_scale
    return jnp.clip(values, -24.0, 24.0).astype(jnp.bfloat16)


def draw_extra_log_decay(key, part):
    chosen = jax.random.uniform(jax.random.fold_in(key, 21), (SEQS, 2 * DRAFT_TOKENS, HEADS)) < 0.15
    losses = jnp.log(jax.random.uniform(jax.random.fold_in(key, 22), (SEQS, 2 * DRAFT_TOKENS, HEADS), minval=0.5, maxval=0.8))
    return jnp.where(chosen, losses, 0.0).astype(jnp.float32)


def set_ends(drawn, key, smallest, top_value):
    shape = drawn.shape
    index_at = [jax.random.randint(jax.random.fold_in(key, axis), (), 0, shape[axis]) for axis in range(len(shape))]
    drawn = drawn.at[tuple(index_at)].set(smallest)
    longest = shape.index(max(shape))
    index_at[longest] = (index_at[longest] + 1) % shape[longest]
    return drawn.at[tuple(index_at)].set(top_value)


def shard_levels(stream_key, extent, shards, low, largest):
    def one(dim, blocks):
        heights = jax.random.uniform(jax.random.fold_in(jax.random.fold_in(stream_key, 6), dim), (blocks,), jnp.float32, low / len(shards), largest / len(shards))
        return jnp.repeat(jnp.exp(heights), extent[dim] // blocks).reshape((-1,) + (1,) * (len(extent) - dim - 1))

    gain = one(*shards[0])
    for cut in shards[1:]:
        gain = gain * one(*cut)
    return gain


def normal_values(stream_key, extent, spread, reach, pieces=(), kind=jnp.bfloat16):
    values = jax.random.normal(stream_key, extent, jnp.float32) * spread
    if len(pieces) > 0:
        values = shard_levels(stream_key, extent, pieces, -0.22, 0.18) * values
    return jnp.clip(values, min=-reach, max=reach).astype(kind)


def setup_inputs(seed: int = 0) -> dict:
    key_of = jax.random.split(jax.random.key(seed), 23)
    hidden_vectors = draw_hidden_vectors(jax.random.fold_in(key_of[22], 71), 0)
    input_norm_gain = jnp.clip(1.0 + 0.18 * jax.random.normal(key_of[1], (D,), jnp.float32), 0.1, 1.9)
    gate_matrix = normal_values(key_of[2], (D, INNER), D ** -0.5, 0.125, ((0, 8), (1, 4)))
    value_matrix = normal_values(key_of[3], (D, INNER), D ** -0.5, 0.125, ((0, 8), (1, 4)))
    write_matrix = normal_values(key_of[4], (D, GROUPS * STATE), D ** -0.5, 0.125, ((0, 8), (1, 4)))
    read_matrix = normal_values(key_of[5], (D, GROUPS * STATE), D ** -0.5, 0.125, ((0, 8), (1, 4)))
    step_matrix = normal_values(key_of[6], (D, HEADS), D ** -0.5, 0.125, ((0, 8), (1, 4)))
    raw_value_rows = normal_values(key_of[7], (SEQS, TAPS - 1 + DRAFT_TOKENS, INNER), 1.0, 6.0, ((0, 8), (2, 4)))
    raw_write_rows = normal_values(key_of[8], (SEQS, TAPS - 1 + DRAFT_TOKENS, GROUPS * STATE), 1.0, 6.0, ((0, 8), (2, 4)))
    raw_read_rows = normal_values(key_of[9], (SEQS, TAPS - 1 + DRAFT_TOKENS, GROUPS * STATE), 1.0, 6.0, ((0, 8), (2, 4)))
    value_filter_taps = normal_values(key_of[10], (TAPS, INNER), TAPS ** -0.5, 3.0, ((1, 4),))
    write_filter_taps = normal_values(key_of[11], (TAPS, GROUPS * STATE), TAPS ** -0.5, 3.0, ((1, 4),))
    read_filter_taps = normal_values(key_of[12], (TAPS, GROUPS * STATE), TAPS ** -0.5, 3.0, ((1, 4),))
    step_size_bias = jnp.clip(-3.0 + 3.0 * jax.random.uniform(key_of[13], (HEADS,), jnp.float32) ** shard_levels(key_of[13], (HEADS,), ((0, 4),), -0.2, 0.2), -3.0, 0.0)
    rate_logarithm = jnp.clip(-4.0 + 4.5 * jax.random.uniform(key_of[14], (HEADS,), jnp.float32) ** shard_levels(key_of[14], (HEADS,), ((0, 4),), -0.2, 0.2), -4.0, 0.5)
    direct_path_gain = jnp.clip(1.0 + 0.18 * jax.random.normal(key_of[15], (HEADS,), jnp.float32), 0.1, 1.9)
    prior_step_preact = normal_values(key_of[16], (SEQS, DRAFT_TOKENS, HEADS), 1.0, 6.0, ((0, 8), (2, 4)), jnp.float32)
    extra_log_decay = draw_extra_log_decay(jax.random.fold_in(key_of[22], 71), 0)
    accepted = set_ends(jax.random.randint(key_of[18], (SEQS,), 0, DRAFT_TOKENS + 1), jax.random.fold_in(key_of[18], 1), 0, DRAFT_TOKENS).astype(jnp.int32)
    prior_state = normal_values(key_of[19], (SEQS, HEADS, HEAD_DIM, STATE), 1.0, 6.0, ((0, 8), (1, 4)), jnp.float32)
    group_norm_gain = jnp.clip(1.0 + 0.18 * jax.random.normal(key_of[20], (INNER,), jnp.float32), 0.1, 1.9)
    output_matrix = normal_values(key_of[21], (INNER, D), INNER ** -0.5, 0.09375, ((0, 4), (1, 8)))
    return dict(hidden_vectors=hidden_vectors, input_norm_gain=input_norm_gain, gate_matrix=gate_matrix, value_matrix=value_matrix, write_matrix=write_matrix, read_matrix=read_matrix, step_matrix=step_matrix, raw_value_rows=raw_value_rows, raw_write_rows=raw_write_rows, raw_read_rows=raw_read_rows, value_filter_taps=value_filter_taps, write_filter_taps=write_filter_taps, read_filter_taps=read_filter_taps, step_size_bias=step_size_bias, rate_logarithm=rate_logarithm, direct_path_gain=direct_path_gain, prior_step_preact=prior_step_preact, extra_log_decay=extra_log_decay, accepted=accepted, prior_state=prior_state, group_norm_gain=group_norm_gain, output_matrix=output_matrix)


epsilon = 1e-06
highest = lax.Precision.HIGHEST

def conv_rows(row_block, taps):
    length_rows = row_block.shape[1] - (TAPS - 1)
    result = jnp.zeros((row_block.shape[0], length_rows, row_block.shape[2]), jnp.float32)
    for tap_index in range(TAPS):
        result = result + row_block[:, tap_index:tap_index + length_rows].astype(jnp.float32) * taps[tap_index].astype(jnp.float32)
    return jax.nn.silu(result)

def resume_state(start_state, values, writes, head_step_size, decay_logarithm, accepted):
    live_mask = (jnp.arange(values.shape[1])[None, :] < accepted[:, None]).astype(jnp.float32)
    kept_decay = decay_logarithm * live_mask[:, :, None]
    total_decay = lax.optimization_barrier(jnp.sum(kept_decay, axis=1))
    tail_decay = total_decay[:, None, :] - jnp.cumsum(kept_decay, axis=1)
    coefficient = live_mask[:, :, None] * jnp.exp(tail_decay) * head_step_size
    added = jnp.einsum('skh,skhp,skhn->shpn', coefficient, values, writes, precision=highest)
    return jnp.exp(total_decay)[:, :, None, None] * start_state + added

def dual_block(values, writes, reads, head_step_size, decay_logarithm, direct_path_gain, start_state):
    cumulative = jnp.cumsum(decay_logarithm, axis=1)
    carried = jnp.exp(cumulative)[..., None] * jnp.einsum('skhn,shpn->skhp', reads, start_state, precision=highest)
    order = jnp.arange(cumulative.shape[1])
    causal = order[:, None] >= order[None, :]
    difference = cumulative[:, :, None, :] - cumulative[:, None, :, :]
    decay_weight = jnp.where(causal[None, :, :, None], jnp.exp(jnp.minimum(difference, 0.0)), 0.0)
    inner_terms = jnp.einsum('sthn,suhn->stuh', reads, writes, precision=highest)
    within = jnp.einsum('stuh,suh,suhp->sthp', inner_terms * decay_weight, head_step_size, values, precision=highest)
    return carried + within + direct_path_gain[None, None, :, None] * values

def mixer_kernel_body(output_gate, fresh_values, fresh_writes, fresh_reads, step_preact, raw_value_rows, raw_write_rows, raw_read_rows, value_filter_taps, write_filter_taps, read_filter_taps, step_size_bias, rate_logarithm, direct_path_gain, prior_step_preact, extra_log_decay, accepted, prior_state, group_norm_gain):
    seq_count = raw_value_rows.shape[0]
    head_count = step_preact.shape[2]
    group_count = fresh_writes.shape[2] // STATE
    per_group = head_count // group_count
    window = accepted[:, None] + jnp.arange(TAPS - 1, dtype=jnp.int32)[None, :]

    def current(row_block, new_rows, taps):
        earlier = jnp.take_along_axis(row_block, window[:, :, None], axis=1)
        return conv_rows(jnp.concatenate([earlier, new_rows], axis=1), taps)
    conv_values = current(raw_value_rows, fresh_values, value_filter_taps).reshape(seq_count, DRAFT_TOKENS, head_count, HEAD_DIM)
    conv_writes = current(raw_write_rows, fresh_writes, write_filter_taps).reshape(seq_count, DRAFT_TOKENS, group_count, STATE)
    conv_reads = current(raw_read_rows, fresh_reads, read_filter_taps).reshape(seq_count, DRAFT_TOKENS, group_count, STATE)
    last_values = conv_rows(raw_value_rows, value_filter_taps).reshape(seq_count, DRAFT_TOKENS, head_count, HEAD_DIM)
    last_writes = conv_rows(raw_write_rows, write_filter_taps).reshape(seq_count, DRAFT_TOKENS, group_count, STATE)
    head_decay_rate = jnp.exp(rate_logarithm)
    head_step_size = jax.nn.softplus(step_preact + step_size_bias)
    decay_logarithm = -head_decay_rate * head_step_size + extra_log_decay[:, DRAFT_TOKENS:]
    prior_step = jax.nn.softplus(prior_step_preact + step_size_bias)
    prior_decay = -head_decay_rate * prior_step + extra_log_decay[:, :DRAFT_TOKENS]
    restored_state = resume_state(prior_state, last_values, jnp.repeat(last_writes, per_group, axis=2), prior_step, prior_decay, accepted)
    mixed_heads = dual_block(conv_values, jnp.repeat(conv_writes, per_group, axis=2), jnp.repeat(conv_reads, per_group, axis=2), head_step_size, decay_logarithm, direct_path_gain, restored_state)
    gated = mixed_heads.reshape(seq_count, DRAFT_TOKENS, -1) * jax.nn.silu(output_gate.astype(jnp.float32))
    group_width = INNER // GROUPS
    grouped = gated.reshape(seq_count, DRAFT_TOKENS, -1, group_width)
    scale = lax.rsqrt(lax.optimization_barrier(jnp.mean(grouped * grouped, axis=-1, keepdims=True)) + epsilon)
    normalized_hidden = (grouped * scale).reshape(seq_count, DRAFT_TOKENS, -1) * group_norm_gain
    return (normalized_hidden.astype(jnp.bfloat16).reshape(seq_count * DRAFT_TOKENS, -1), restored_state)

def reference(hidden_vectors, input_norm_gain, gate_matrix, value_matrix, write_matrix, read_matrix, step_matrix, raw_value_rows, raw_write_rows, raw_read_rows, value_filter_taps, write_filter_taps, read_filter_taps, step_size_bias, rate_logarithm, direct_path_gain, prior_step_preact, extra_log_decay, accepted, prior_state, group_norm_gain, output_matrix):
    floats_in = hidden_vectors.astype(jnp.float32)
    inverse = lax.rsqrt(lax.optimization_barrier(jnp.mean(floats_in * floats_in, axis=1)) + epsilon)[:, None]
    scaled = (floats_in * input_norm_gain).astype(jnp.bfloat16)

    def project(weight):
        return inverse * jnp.dot(scaled, weight, preferred_element_type=jnp.float32)

    def shaped(matrix):
        return matrix.reshape(SEQS, DRAFT_TOKENS, -1)
    output_gate = shaped(project(gate_matrix).astype(jnp.bfloat16))
    fresh_values = shaped(project(value_matrix).astype(jnp.bfloat16))
    fresh_writes = shaped(project(write_matrix).astype(jnp.bfloat16))
    fresh_reads = shaped(project(read_matrix).astype(jnp.bfloat16))
    step_preact = shaped(project(step_matrix))
    normalized_hidden, restored_state = mixer_kernel_body(output_gate, fresh_values, fresh_writes, fresh_reads, step_preact, raw_value_rows, raw_write_rows, raw_read_rows, value_filter_taps, write_filter_taps, read_filter_taps, step_size_bias, rate_logarithm, direct_path_gain, prior_step_preact, extra_log_decay, accepted, prior_state, group_norm_gain)
    block_width = INNER // N_TP
    mixer_out = jnp.zeros((TOKENS, D), jnp.float32)
    for block_index in range(N_TP):
        lower = block_index * block_width
        partial_value = jnp.dot(normalized_hidden[:, lower:lower + block_width], output_matrix[lower:lower + block_width], preferred_element_type=jnp.float32).astype(jnp.bfloat16)
        partial_value = lax.optimization_barrier(partial_value)
        mixer_out = mixer_out + partial_value.astype(jnp.float32)
    return (mixer_out.astype(jnp.bfloat16), restored_state)
```

```python
import functools

import jax
import jax.numpy as jnp
from jax import lax
from jax.experimental import pallas as pl
from jax.experimental.pallas import tpu as pltpu
from jax.sharding import PartitionSpec as P

epsilon = 1e-06
lanes = 128
half_lanes = lanes // 2


VMEM = pl.BlockSpec(memory_space=pltpu.VMEM)
SMEM = pl.BlockSpec(memory_space=pltpu.SMEM)
ANY = pl.BlockSpec(memory_space=pl.ANY)
f32 = jnp.float32
bf16 = jnp.bfloat16


def reverse_bits(index, width):
    result = index * 0
    for bit in range(width):
        result = result | (((index >> bit) & 1) << (width - 1 - bit))
    return result


def split_pair(x):
    high = x.astype(bf16).astype(f32)
    return high, x - high


def fold_aux(aux):
    lane = lax.broadcasted_iota(jnp.int32, aux.shape, 1)
    return jnp.where(lane < half_lanes, aux + pltpu.roll(aux, half_lanes, 1), 0.0)


def pair_aux(aux):
    high, low = split_pair(aux)
    return (high + pltpu.roll(low, half_lanes, 1)).astype(bf16)


def silu(x):
    return x / (1.0 + jnp.exp(-x))


def softplus(x):
    return jnp.maximum(x, 0.0) + jnp.log1p(jnp.exp(-jnp.abs(x)))


def expander(heads, width):
    row = lax.broadcasted_iota(jnp.int32, (heads, width), 0)
    column = lax.broadcasted_iota(jnp.int32, (heads, width), 1)
    return (column // (width // heads) == row).astype(f32).astype(bf16)


def expand(x, matrix):
    rows = x.shape[0]
    high, low = split_pair(x)
    both = jnp.concatenate([high, low], axis=0).astype(bf16)
    wide = jnp.dot(both, matrix, preferred_element_type=f32)
    return wide[:rows] + wide[rows:]


def project_body(
    stages, hidden_ref, gain_ref, step_ref, *refs
):
    weights, (keep_ref, send_ref), buffers, (aux_ref, sems) = refs[:4], refs[4:6], refs[6:10], refs[10:]
    copies = [
        pltpu.make_async_copy(weight, buffer, sems.at[i])
        for i, (weight, buffer) in enumerate(zip(weights, buffers))
    ]
    for copy in copies:
        copy.start()
    me = lax.axis_index("kv")
    blocks = [hidden_ref[reverse_bits(p, stages) ^ me] for p in range(1 << stages)]
    floats_in = jnp.concatenate([b.astype(f32) for b in blocks], axis=0)
    squares = jnp.sum(floats_in * floats_in, axis=1, keepdims=True)
    scaled = (floats_in * gain_ref[...]).astype(bf16)
    heads = step_ref.shape[1]
    half = floats_in.shape[0] // 2
    aux_ref[...] = jnp.zeros_like(aux_ref)
    aux_ref[:, :heads] = jnp.dot(scaled, step_ref[...], preferred_element_type=f32)
    lane = lax.broadcasted_iota(jnp.int32, aux_ref.shape, 1)
    aux = jnp.where(lane == heads, squares, aux_ref[...])
    start = keep_ref.shape[1] - lanes
    keep_ref[:, start:] = aux[:half]
    send_ref[:, start:] = pair_aux(aux[half:])
    start = 0
    for copy, buffer in zip(copies, buffers):
        copy.wait()
        part = jnp.dot(scaled, buffer[...], preferred_element_type=f32)
        stop = start + buffer.shape[1]
        keep_ref[:, start:stop] = part[:half]
        send_ref[:, start:stop] = part[half:].astype(bf16)
        start = stop


def combine_body(keep_ref, recv_ref, next_ref, send_ref):
    half = next_ref.shape[0]
    start = keep_ref.shape[1] - lanes
    total = keep_ref[:, :start] + recv_ref[:, :start].astype(f32)
    next_ref[:, :start] = total[:half]
    send_ref[:, :start] = total[half:].astype(bf16)
    aux = fold_aux(keep_ref[:, start:] + recv_ref[:, start:].astype(f32))
    next_ref[:, start:] = aux[:half]
    send_ref[:, start:] = pair_aux(aux[half:])


def resume_body(
    accepted_ref,
    raw_value_ref,
    raw_write_ref,
    raw_read_ref,
    value_taps_ref,
    write_taps_ref,
    read_taps_ref,
    bias_ref,
    rate_ref,
    prior_step_ref,
    extra_ref,
    state_in,
    state_out,
    high_ref,
    low_ref,
    pre_ref,
    state_ref,
    raw_ref,
    window_ref,
    taps_ref,
    last_ref,
    in_sems,
    out_sems,
):
    seqs, heads, head_dim, width_n = state_ref.shape
    inner = heads * head_dim
    writes = raw_write_ref.shape[2]
    groups = writes // width_n
    per_group = heads // groups
    drafts = prior_step_ref.shape[1]
    taps = value_taps_ref.shape[0]
    places = [(s, g) for s in range(seqs) for g in range(groups)]

    def moving(s, g, source, target, sems):
        where = (s, pl.ds(g * per_group, per_group))
        return pltpu.make_async_copy(source.at[where], target.at[where], sems.at[s, g])

    for s, g in places:
        moving(s, g, state_in, state_ref, in_sems).start()
    cuts = (0, inner, inner + writes, inner + 2 * writes)
    roles = (
        (raw_value_ref, value_taps_ref),
        (raw_write_ref, write_taps_ref),
        (raw_read_ref, read_taps_ref),
    )
    for i, (_, tap_ref) in enumerate(roles):
        taps_ref[:, cuts[i] : cuts[i + 1]] = tap_ref[...].astype(f32)
    raw_rows = raw_value_ref.shape[1]
    raw_ref[...] = jnp.zeros_like(raw_ref)
    window_ref[...] = jnp.zeros_like(window_ref)
    for s in range(seqs):
        count = accepted_ref[s]
        for i, (row_ref, _) in enumerate(roles):
            raw_ref[:raw_rows, cuts[i] : cuts[i + 1]] = row_ref[s].astype(f32)
        last = taps_ref[0:1, : cuts[2]] * raw_ref[0:drafts, : cuts[2]]
        for j in range(1, taps):
            last = last + taps_ref[j : j + 1, : cuts[2]] * raw_ref[j : j + drafts, : cuts[2]]
        last_ref[s * drafts : (s + 1) * drafts, :] = silu(last)
        window = raw_ref[0 : taps - 1, :]
        for a in range(1, drafts + 1):
            window = jnp.where(count == a, raw_ref[a : a + taps - 1, :], window)
        window_ref[: taps - 1, :] = window
        pre = taps_ref[0:1, :] * window_ref[0:drafts, :]
        for j in range(1, taps - 1):
            pre = pre + taps_ref[j : j + 1, :] * window_ref[j : j + drafts, :]
        pre_ref[s * drafts : (s + 1) * drafts, :] = pre
    rows = seqs * drafts
    row = lax.broadcasted_iota(jnp.int32, (rows, heads), 0)
    order = row % drafts
    count_of = jnp.full((rows, heads), accepted_ref[0], jnp.int32)
    for s in range(1, seqs):
        count_of = jnp.where(row >= s * drafts, accepted_ref[s], count_of)
    live = (order < count_of).astype(f32)
    preact = jnp.concatenate([prior_step_ref[s] for s in range(seqs)], axis=0)
    extra = jnp.concatenate([extra_ref[s, :drafts] for s in range(seqs)], axis=0)
    step = softplus(preact + bias_ref[...])
    kept = live * (extra - jnp.exp(rate_ref[...]) * step)
    tail = jnp.zeros_like(kept)
    for d in range(1, drafts):
        tail = tail + jnp.where(order + d < drafts, pltpu.roll(kept, rows - d, 0), 0.0)
    carry = jnp.exp(kept + tail)
    coefficient = expand(live * jnp.exp(tail) * step, expander(heads, inner))
    weighted = coefficient * last_ref[:, :inner]
    weighted_high, weighted_low = split_pair(weighted)
    write_high, write_low = split_pair(last_ref[:, inner:])
    wide_row = lax.broadcasted_iota(jnp.int32, (rows, inner), 0)
    right = jnp.concatenate([write_high, write_high, write_low, write_low], axis=0).astype(bf16)
    span = per_group * head_dim
    for s in range(seqs):
        own = (wide_row >= s * drafts) & (wide_row < (s + 1) * drafts)
        high = jnp.where(own, weighted_high, 0.0)
        low = jnp.where(own, weighted_low, 0.0)
        left = jnp.concatenate([high, low, high, low], axis=0).astype(bf16)
        for g in range(groups):
            added = lax.dot_general(
                left[:, g * span : (g + 1) * span],
                right[:, g * width_n : (g + 1) * width_n],
                (((0,), (0,)), ((), ())),
                preferred_element_type=f32,
            )
            moving(s, g, state_in, state_ref, in_sems).wait()
            for i in range(per_group):
                h = g * per_group + i
                factor = carry[s * drafts : s * drafts + 1, h : h + 1]
                fresh = factor * state_ref[s, h] + added[i * head_dim : (i + 1) * head_dim]
                state_ref[s, h] = fresh
                fresh_high, fresh_low = split_pair(fresh)
                high_ref[s, h * head_dim : (h + 1) * head_dim, :] = fresh_high.astype(bf16)
                low_ref[s, h * head_dim : (h + 1) * head_dim, :] = fresh_low.astype(bf16)
            moving(s, g, state_ref, state_out, out_sems).start()
    for s, g in places:
        moving(s, g, state_ref, state_out, out_sems).wait()


def mixer_body(
    features,
    keep_ref,
    recv_ref,
    pre_ref,
    value_taps_ref,
    write_taps_ref,
    read_taps_ref,
    bias_ref,
    rate_ref,
    direct_ref,
    extra_ref,
    high_ref,
    low_ref,
    norm_gain_ref,
    out_ref,
):
    rows, inner = out_ref.shape
    heads = bias_ref.shape[1]
    seqs = extra_ref.shape[0]
    drafts = rows // seqs
    taps = value_taps_ref.shape[0]
    width_n = high_ref.shape[2]
    writes = write_taps_ref.shape[1]
    groups = writes // width_n
    span = inner // groups
    main = keep_ref.shape[1] - lanes
    order_of = lambda shape: lax.broadcasted_iota(jnp.int32, shape, 0) % drafts

    def back(x, d):
        if d == 0:
            return x
        return jnp.where(order_of(x.shape) >= d, pltpu.roll(x, d, 0), 0.0)

    aux = fold_aux(keep_ref[:, main:] + recv_ref[:, main:].astype(f32))
    inverse = lax.rsqrt(aux[:, heads : heads + 1] / features + epsilon)
    step_pre = aux[:, :heads] * inverse

    def role(start, stop):
        return inverse * (keep_ref[:, start:stop] + recv_ref[:, start:stop].astype(f32))

    def convolved(start, width, tap_ref):
        fresh = role(inner + start, inner + start + width)
        total = pre_ref[:, start : start + width]
        for d in range(taps):
            total = total + tap_ref[taps - 1 - d : taps - d, :].astype(f32) * back(fresh, d)
        return silu(total)

    reads = convolved(inner + writes, writes, read_taps_ref)
    new_writes = convolved(inner, writes, write_taps_ref)

    step = softplus(step_pre + bias_ref[...])
    extra = jnp.concatenate([extra_ref[s, drafts:] for s in range(seqs)], axis=0)
    log_decay = extra - jnp.exp(rate_ref[...]) * step
    total_decay = log_decay
    for d in range(1, drafts):
        total_decay = total_decay + back(log_decay, d)
    head = lax.broadcasted_iota(jnp.int32, (rows, heads), 1)
    small = [jnp.exp(total_decay)]
    for d in range(drafts):
        products = reads * back(new_writes, d)
        inner_term = jnp.zeros((rows, heads), f32)
        for g in range(groups):
            dot = jnp.sum(products[:, g * width_n : (g + 1) * width_n], axis=1, keepdims=True)
            inner_term = jnp.where(head // (heads // groups) == g, dot, inner_term)
        term = inner_term * back(step, d)
        if d == 0:
            term = term + direct_ref[...]
        else:
            difference = jnp.minimum(total_decay - back(total_decay, d), 0.0)
            term = term * jnp.where(order_of(term.shape) >= d, jnp.exp(difference), 0.0)
        small.append(term)
    wide = expand(jnp.concatenate(small, axis=0), expander(heads, inner))

    reads_high, reads_low = split_pair(reads)
    reads_both = jnp.concatenate([reads_high, reads_low], axis=0).astype(bf16)
    across = (((1,), (1,)), ((), ()))
    values = convolved(0, inner, value_taps_ref)
    for g in range(groups):
        columns = slice(g * span, (g + 1) * span)
        left = reads_both[:, g * width_n : (g + 1) * width_n]
        carried = None
        for s in range(seqs):
            product = lax.dot_general(
                left, high_ref[s, columns, :], across, preferred_element_type=f32
            )
            fine = lax.dot_general(
                left[:rows], low_ref[s, columns, :], across, preferred_element_type=f32
            )
            product = product[:rows] + product[rows:] + fine
            if carried is None:
                carried = product
            else:
                row = lax.broadcasted_iota(jnp.int32, product.shape, 0)
                carried = jnp.where(row >= s * drafts, product, carried)
        mixed = carried * wide[:rows, columns]
        for d in range(drafts):
            mixed = mixed + wide[(d + 1) * rows : (d + 2) * rows, columns] * back(
                values[:, columns], d
            )
        gated = mixed * silu(role(g * span, (g + 1) * span))
        scale = lax.rsqrt(jnp.mean(gated * gated, axis=1, keepdims=True) + epsilon)
        out_ref[:, columns] = (gated * scale * norm_gain_ref[:, columns]).astype(bf16)


def output_body(stages, tp_stages, own_ref, recv_ref, weight_ref, keep_ref, send_ref, sorted_ref):
    me = lax.axis_index("kv")
    tp_me = lax.axis_index("tp")
    blocks = 1 << stages
    per_tp = blocks >> tp_stages
    rows = sorted_ref.shape[1]
    half = blocks // 2
    for part, ref in enumerate((own_ref, recv_ref)):
        product = jnp.dot(ref[...], weight_ref[...], preferred_element_type=f32)
        for p in range(half):
            block = reverse_bits(part * half + p, stages) ^ me
            place = reverse_bits((block // per_tp) ^ tp_me, tp_stages) * per_tp + block % per_tp
            sorted_ref[place] = product[p * rows : (p + 1) * rows]
    for p in range(half):
        keep_ref[p * rows : (p + 1) * rows, :] = sorted_ref[p].astype(bf16).astype(f32)
        send_ref[p * rows : (p + 1) * rows, :] = sorted_ref[half + p].astype(bf16)


def per_device(
    kv_size,
    tp_size,
    hidden_vectors,
    input_norm_gain,
    gate_matrix,
    value_matrix,
    write_matrix,
    read_matrix,
    step_matrix,
    raw_value_rows,
    raw_write_rows,
    raw_read_rows,
    value_filter_taps,
    write_filter_taps,
    read_filter_taps,
    step_size_bias,
    rate_logarithm,
    direct_path_gain,
    prior_step_preact,
    extra_log_decay,
    accepted,
    prior_state,
    group_norm_gain,
    output_matrix,
):
    stages = kv_size.bit_length() - 1
    tp_stages = tp_size.bit_length() - 1
    tokens, features = hidden_vectors.shape
    rows = tokens // kv_size
    seqs, heads, head_dim, width_n = prior_state.shape
    inner = heads * head_dim
    weights = (gate_matrix, value_matrix, write_matrix, read_matrix)
    width = sum(w.shape[1] for w in weights) + lanes
    swap = lambda x, axis, size, bit: lax.ppermute(x, axis, [(i, i ^ bit) for i in range(size)])
    line = lambda x: x.reshape(1, -1)
    shape = jax.ShapeDtypeStruct

    half = tokens // 2
    keep, send = pl.pallas_call(
        functools.partial(project_body, stages),
        out_shape=(shape((half, width), f32), shape((half, width), bf16)),
        in_specs=[VMEM] * 3 + [ANY] * 4,
        out_specs=(VMEM, VMEM),
        scratch_shapes=[pltpu.VMEM(w.shape, w.dtype) for w in weights]
        + [pltpu.VMEM((tokens, lanes), f32), pltpu.SemaphoreType.DMA((4,))],
        name="project",
    )(
        hidden_vectors.reshape(kv_size, rows, features),
        line(input_norm_gain),
        step_matrix,
        *weights,
    )

    groups = raw_write_rows.shape[2] // width_n
    columns = inner + 2 * groups * width_n
    bias, rate = line(step_size_bias), line(rate_logarithm)
    filters = (value_filter_taps, write_filter_taps, read_filter_taps)
    taps = value_filter_taps.shape[0]
    resumed, high, low, pre = pl.pallas_call(
        resume_body,
        out_shape=(
            shape(prior_state.shape, f32),
            shape((seqs, inner, width_n), bf16),
            shape((seqs, inner, width_n), bf16),
            shape((rows, columns), f32),
        ),
        in_specs=[SMEM] + [VMEM] * 10 + [ANY],
        out_specs=(ANY, VMEM, VMEM, VMEM),
        scratch_shapes=[
            pltpu.VMEM(prior_state.shape, f32),
            pltpu.VMEM((8, columns), f32),
            pltpu.VMEM((8, columns), f32),
            pltpu.VMEM((taps, columns), f32),
            pltpu.VMEM((rows, inner + groups * width_n), f32),
            pltpu.SemaphoreType.DMA((seqs, groups)),
            pltpu.SemaphoreType.DMA((seqs, groups)),
        ],
        cost_estimate=pl.CostEstimate(flops=40_000_000, bytes_accessed=4_000_000, transcendentals=0),
        name="resume",
    )(
        accepted,
        raw_value_rows,
        raw_write_rows,
        raw_read_rows,
        *filters,
        bias,
        rate,
        prior_step_preact,
        extra_log_decay,
        prior_state,
    )

    for stage in range(stages):
        recv = swap(send, "kv", kv_size, 1 << stage)
        if stage < stages - 1:
            half = half // 2
            keep, send = pl.pallas_call(
                combine_body,
                out_shape=(shape((half, width), f32), shape((half, width), bf16)),
                in_specs=[VMEM, VMEM],
                out_specs=(VMEM, VMEM),
                name="combine",
            )(keep, recv)

    normed = pl.pallas_call(
        functools.partial(mixer_body, features * kv_size),
        out_shape=shape((rows, inner), bf16),
        in_specs=[VMEM] * 13,
        out_specs=VMEM,
        name="mixer",
    )(
        keep,
        recv,
        pre,
        *filters,
        bias,
        rate,
        line(direct_path_gain),
        extra_log_decay,
        high,
        low,
        line(group_norm_gain),
    )

    for stage in reversed(range(stages)):
        recv = swap(normed, "kv", kv_size, 1 << stage)
        if stage > 0:
            normed = jnp.concatenate([normed, recv], axis=0)

    half = tokens // 2
    out_width = output_matrix.shape[1]
    keep, send = pl.pallas_call(
        functools.partial(output_body, stages, tp_stages),
        out_shape=(shape((half, out_width), f32), shape((half, out_width), bf16)),
        in_specs=[VMEM] * 3,
        out_specs=(VMEM, VMEM),
        scratch_shapes=[pltpu.VMEM((kv_size, rows, out_width), f32)],
        name="output",
    )(normed, recv, output_matrix)
    for stage in range(tp_stages):
        total = keep + swap(send, "tp", tp_size, 1 << stage).astype(f32)
        half = half // 2
        if stage < tp_stages - 1:
            keep, send = total[:half], total[half:]
    return total.astype(bf16), resumed


def solution(mesh):
    placed = (
        P(None, "kv"),
        P("kv"),
        P("kv", "tp"),
        P("kv", "tp"),
        P("kv", "tp"),
        P("kv", "tp"),
        P("kv", "tp"),
        P("kv", None, "tp"),
        P("kv", None, "tp"),
        P("kv", None, "tp"),
        P(None, "tp"),
        P(None, "tp"),
        P(None, "tp"),
        P("tp"),
        P("tp"),
        P("tp"),
        P("kv", None, "tp"),
        P("kv", None, "tp"),
        P("kv"),
        P("kv", "tp", None, None),
        P("tp"),
        P("tp", "kv"),
    )
    return jax.shard_map(
        functools.partial(per_device, mesh.shape["kv"], mesh.shape["tp"]),
        mesh=mesh,
        in_specs=placed,
        out_specs=(P("tp", "kv"), P("kv", "tp", None, None)),
        check_vma=False,
    )
```

```python
import functools

import jax
import jax.numpy as jnp
from jax import lax
from jax.experimental import pallas as pl
from jax.experimental.pallas import tpu as pltpu
from jax.sharding import PartitionSpec as P

epsilon = 1e-06
lanes = 128
half_lanes = lanes // 2


VMEM = pl.BlockSpec(memory_space=pltpu.VMEM)
SMEM = pl.BlockSpec(memory_space=pltpu.SMEM)
ANY = pl.BlockSpec(memory_space=pl.ANY)
PARAMS = pltpu.CompilerParams(vmem_limit_bytes=24 * 2**20)
f32 = jnp.float32
bf16 = jnp.bfloat16


def reverse_bits(index, width):
    result = index * 0
    for bit in range(width):
        result = result | (((index >> bit) & 1) << (width - 1 - bit))
    return result


def split_pair(x):
    high = x.astype(bf16).astype(f32)
    return high, x - high


def fold_aux(aux):
    lane = lax.broadcasted_iota(jnp.int32, aux.shape, 1)
    return jnp.where(lane < half_lanes, aux + pltpu.roll(aux, half_lanes, 1), 0.0)


def pair_aux(aux):
    high, low = split_pair(aux)
    return (high + pltpu.roll(low, half_lanes, 1)).astype(bf16)


def silu(x):
    return x / (1.0 + jnp.exp(-x))


def softplus(x):
    return jnp.maximum(x, 0.0) + jnp.log1p(jnp.exp(-jnp.abs(x)))


def expander(heads, width):
    row = lax.broadcasted_iota(jnp.int32, (heads, width), 0)
    column = lax.broadcasted_iota(jnp.int32, (heads, width), 1)
    return (column // (width // heads) == row).astype(f32).astype(bf16)


def expand(x, matrix):
    rows = x.shape[0]
    high, low = split_pair(x)
    both = jnp.concatenate([high, low], axis=0).astype(bf16)
    wide = jnp.dot(both, matrix, preferred_element_type=f32)
    return wide[:rows] + wide[rows:]


def project_body(stages, *refs):
    sources, (keep_ref, send_ref), buffers, (aux_ref, sems) = refs[:7], refs[7:9], refs[9:16], refs[16:]
    copies = [
        pltpu.make_async_copy(source, buffer, sems.at[i])
        for i, (source, buffer) in enumerate(zip(sources, buffers))
    ]
    for copy in copies:
        copy.start()
    hidden_ref, gain_ref, step_ref = buffers[:3]
    me = lax.axis_index("kv")
    for copy in copies[:3]:
        copy.wait()
    blocks = [hidden_ref[reverse_bits(p, stages) ^ me] for p in range(1 << stages)]
    floats_in = jnp.concatenate([b.astype(f32) for b in blocks], axis=0)
    squares = jnp.sum(floats_in * floats_in, axis=1, keepdims=True)
    scaled = (floats_in * gain_ref[...]).astype(bf16)
    heads = step_ref.shape[0]
    half = floats_in.shape[0] // 2
    aux_ref[...] = jnp.zeros_like(aux_ref)
    aux_ref[:, :heads] = lax.dot_general(
        scaled, step_ref[...], (((1,), (1,)), ((), ())), preferred_element_type=f32
    )
    lane = lax.broadcasted_iota(jnp.int32, aux_ref.shape, 1)
    aux = jnp.where(lane == heads, squares, aux_ref[...])
    start = keep_ref.shape[1] - lanes
    keep_ref[:, start:] = aux[:half]
    send_ref[:, start:] = pair_aux(aux[half:])
    start = 0
    for copy, buffer in zip(copies[3:], buffers[3:]):
        copy.wait()
        part = jnp.dot(scaled, buffer[...], preferred_element_type=f32)
        stop = start + buffer.shape[1]
        keep_ref[:, start:stop] = part[:half]
        send_ref[:, start:stop] = part[half:].astype(bf16)
        start = stop


def combine_body(keep_ref, recv_ref, _, next_ref, send_ref):
    half = next_ref.shape[0]
    start = keep_ref.shape[1] - lanes
    total = keep_ref[:, :start] + recv_ref[:, :start].astype(f32)
    next_ref[:, :start] = total[:half]
    send_ref[:, :start] = total[half:].astype(bf16)
    aux = fold_aux(keep_ref[:, start:] + recv_ref[:, start:].astype(f32))
    next_ref[:, start:] = aux[:half]
    send_ref[:, start:] = pair_aux(aux[half:])


def resume_body(
    accepted_ref,
    raw_value_ref,
    raw_write_ref,
    raw_read_ref,
    value_taps_ref,
    write_taps_ref,
    read_taps_ref,
    bias_ref,
    rate_ref,
    direct_ref,
    norm_gain_ref,
    prior_step_ref,
    extra_ref,
    state_in,
    state_out,
    high_ref,
    low_ref,
    pre_ref,
    small_ref,
    gain_ref,
    state_ref,
    raw_ref,
    window_ref,
    taps_ref,
    last_ref,
    in_sems,
    out_sems,
):
    seqs, heads, head_dim, width_n = state_ref.shape
    inner = heads * head_dim
    writes = raw_write_ref.shape[2]
    groups = writes // width_n
    per_group = heads // groups
    drafts = prior_step_ref.shape[1]
    taps = value_taps_ref.shape[0]
    places = [(s, g) for s in range(seqs) for g in range(groups)]

    def moving(s, g, source, target, sems):
        where = (s, pl.ds(g * per_group, per_group))
        return pltpu.make_async_copy(source.at[where], target.at[where], sems.at[s, g])

    for s, g in places:
        moving(s, g, state_in, state_ref, in_sems).start()
    cuts = (0, inner, inner + writes, inner + 2 * writes)
    roles = (
        (raw_value_ref, value_taps_ref),
        (raw_write_ref, write_taps_ref),
        (raw_read_ref, read_taps_ref),
    )
    for i, (_, tap_ref) in enumerate(roles):
        taps_ref[:, cuts[i] : cuts[i + 1]] = tap_ref[...].astype(f32)
    raw_rows = raw_value_ref.shape[0]
    raw_ref[...] = jnp.zeros_like(raw_ref)
    window_ref[...] = jnp.zeros_like(window_ref)
    for j in range(raw_rows):
        for i, (row_ref, _) in enumerate(roles):
            both = row_ref[j].astype(f32)
            for s in range(seqs):
                raw_ref[s, j : j + 1, cuts[i] : cuts[i + 1]] = both[s : s + 1]
    for s in range(seqs):
        count = accepted_ref[s]
        last = taps_ref[0:1, : cuts[2]] * raw_ref[s, 0:drafts, : cuts[2]]
        for j in range(1, taps):
            last = last + taps_ref[j : j + 1, : cuts[2]] * raw_ref[s, j : j + drafts, : cuts[2]]
        last_ref[s * drafts : (s + 1) * drafts, :] = silu(last)
        window = raw_ref[s, 0 : taps - 1, :]
        for a in range(1, drafts + 1):
            window = jnp.where(count == a, raw_ref[s, a : a + taps - 1, :], window)
        window_ref[: taps - 1, :] = window
        pre = taps_ref[0:1, :] * window_ref[0:drafts, :]
        for j in range(1, taps - 1):
            pre = pre + taps_ref[j : j + 1, :] * window_ref[j : j + drafts, :]
        pre_ref[0, s * drafts : (s + 1) * drafts, :] = pre
    rows = seqs * drafts
    wide_order = lax.broadcasted_iota(jnp.int32, (rows, cuts[3]), 0) % drafts
    for d in range(taps):
        pre_ref[d + 1] = jnp.where(wide_order >= d, taps_ref[taps - 1 - d : taps - d, :], 0.0)
    gain_ref[...] = norm_gain_ref[...]
    small_ref[0] = jnp.broadcast_to(bias_ref[...], (rows, heads))
    small_ref[1] = jnp.broadcast_to(jnp.exp(rate_ref[...]), (rows, heads))
    small_ref[2] = jnp.broadcast_to(direct_ref[...], (rows, heads))
    small_ref[3] = jnp.concatenate([extra_ref[s, drafts:] for s in range(seqs)], axis=0)
    row = lax.broadcasted_iota(jnp.int32, (rows, heads), 0)
    order = row % drafts
    count_of = jnp.full((rows, heads), accepted_ref[0], jnp.int32)
    for s in range(1, seqs):
        count_of = jnp.where(row >= s * drafts, accepted_ref[s], count_of)
    live = (order < count_of).astype(f32)
    preact = jnp.concatenate([prior_step_ref[s] for s in range(seqs)], axis=0)
    extra = jnp.concatenate([extra_ref[s, :drafts] for s in range(seqs)], axis=0)
    step = softplus(preact + bias_ref[...])
    kept = live * (extra - jnp.exp(rate_ref[...]) * step)
    tail = jnp.zeros_like(kept)
    for d in range(1, drafts):
        tail = tail + jnp.where(order + d < drafts, pltpu.roll(kept, rows - d, 0), 0.0)
    carry = jnp.exp(kept + tail)
    coefficient = expand(live * jnp.exp(tail) * step, expander(heads, inner))
    weighted = coefficient * last_ref[:, :inner]
    weighted_high, weighted_low = split_pair(weighted)
    write_high, write_low = split_pair(last_ref[:, inner:])
    wide_row = lax.broadcasted_iota(jnp.int32, (rows, inner), 0)
    right = jnp.concatenate([write_high, write_high, write_low, write_low], axis=0).astype(bf16)
    span = per_group * head_dim
    for s in range(seqs):
        own = (wide_row >= s * drafts) & (wide_row < (s + 1) * drafts)
        high = jnp.where(own, weighted_high, 0.0)
        low = jnp.where(own, weighted_low, 0.0)
        left = jnp.concatenate([high, low, high, low], axis=0).astype(bf16)
        for g in range(groups):
            added = lax.dot_general(
                left[:, g * span : (g + 1) * span],
                right[:, g * width_n : (g + 1) * width_n],
                (((0,), (0,)), ((), ())),
                preferred_element_type=f32,
            )
            moving(s, g, state_in, state_ref, in_sems).wait()
            for i in range(per_group):
                h = g * per_group + i
                factor = carry[s * drafts : s * drafts + 1, h : h + 1]
                fresh = factor * state_ref[s, h] + added[i * head_dim : (i + 1) * head_dim]
                state_ref[s, h] = fresh
                fresh_high, fresh_low = split_pair(fresh)
                high_ref[s, h * head_dim : (h + 1) * head_dim, :] = fresh_high.astype(bf16)
                low_ref[s, h * head_dim : (h + 1) * head_dim, :] = fresh_low.astype(bf16)
            moving(s, g, state_ref, state_out, out_sems).start()
    for s, g in places:
        moving(s, g, state_ref, state_out, out_sems).wait()


def mixer_body(
    features,
    keep_ref,
    recv_ref,
    pre_ref,
    small_ref,
    high_ref,
    low_ref,
    norm_gain_ref,
    out_ref,
):
    rows, inner = out_ref.shape
    heads = small_ref.shape[2]
    seqs, _, width_n = high_ref.shape
    drafts = rows // seqs
    taps = pre_ref.shape[0] - 1
    writes = (pre_ref.shape[2] - inner) // 2
    groups = writes // width_n
    span = inner // groups
    main = keep_ref.shape[1] - lanes
    order_of = lambda shape: lax.broadcasted_iota(jnp.int32, shape, 0) % drafts

    def back(x, d):
        if d == 0:
            return x
        return jnp.where(order_of(x.shape) >= d, pltpu.roll(x, d, 0), 0.0)

    aux = fold_aux(keep_ref[:, main:] + recv_ref[:, main:].astype(f32))
    inverse = lax.rsqrt(aux[:, heads : heads + 1] / features + epsilon)
    step_pre = aux[:, :heads] * inverse

    def role(start, stop):
        return inverse * (keep_ref[:, start:stop] + recv_ref[:, start:stop].astype(f32))

    def convolved(start, width):
        fresh = role(inner + start, inner + start + width)
        total = pre_ref[0, :, start : start + width]
        for d in range(taps):
            shifted = fresh if d == 0 else pltpu.roll(fresh, d, 0)
            total = total + pre_ref[d + 1, :, start : start + width] * shifted
        return silu(total)

    reads = convolved(inner + writes, writes)
    new_writes = convolved(inner, writes)

    step = softplus(step_pre + small_ref[0])
    log_decay = small_ref[3] - small_ref[1] * step
    total_decay = log_decay
    for d in range(1, drafts):
        total_decay = total_decay + back(log_decay, d)
    head = lax.broadcasted_iota(jnp.int32, (rows, heads), 1)
    small = [jnp.exp(total_decay)]
    for d in range(drafts):
        products = reads * back(new_writes, d)
        inner_term = jnp.zeros((rows, heads), f32)
        for g in range(groups):
            dot = jnp.sum(products[:, g * width_n : (g + 1) * width_n], axis=1, keepdims=True)
            inner_term = jnp.where(head // (heads // groups) == g, dot, inner_term)
        term = inner_term * back(step, d)
        if d == 0:
            term = term + small_ref[2]
        else:
            difference = jnp.minimum(total_decay - back(total_decay, d), 0.0)
            term = term * jnp.where(order_of(term.shape) >= d, jnp.exp(difference), 0.0)
        small.append(term)
    wide = expand(jnp.concatenate(small, axis=0), expander(heads, inner))

    reads_high, reads_low = split_pair(reads)
    reads_both = jnp.concatenate([reads_high, reads_low], axis=0).astype(bf16)
    across = (((1,), (1,)), ((), ()))
    values = convolved(0, inner)
    for g in range(groups):
        columns = slice(g * span, (g + 1) * span)
        left = reads_both[:, g * width_n : (g + 1) * width_n]
        carried = None
        for s in range(seqs):
            product = lax.dot_general(
                left, high_ref[s, columns, :], across, preferred_element_type=f32
            )
            fine = lax.dot_general(
                left[:rows], low_ref[s, columns, :], across, preferred_element_type=f32
            )
            product = product[:rows] + product[rows:] + fine
            if carried is None:
                carried = product
            else:
                row = lax.broadcasted_iota(jnp.int32, product.shape, 0)
                carried = jnp.where(row >= s * drafts, product, carried)
        mixed = carried * wide[:rows, columns]
        for d in range(drafts):
            mixed = mixed + wide[(d + 1) * rows : (d + 2) * rows, columns] * back(
                values[:, columns], d
            )
        gated = mixed * silu(role(g * span, (g + 1) * span))
        scale = lax.rsqrt(jnp.mean(gated * gated, axis=1, keepdims=True) + epsilon)
        out_ref[:, columns] = (gated * scale * norm_gain_ref[:, columns]).astype(bf16)


def output_body(stages, tp_stages, own_ref, recv_ref, weight_ref, keep_ref, send_ref, sorted_ref):
    me = lax.axis_index("kv")
    tp_me = lax.axis_index("tp")
    blocks = 1 << stages
    per_tp = blocks >> tp_stages
    rows = sorted_ref.shape[1]
    half = blocks // 2
    for part, ref in enumerate((own_ref, recv_ref)):
        product = jnp.dot(ref[...], weight_ref[...], preferred_element_type=f32)
        for p in range(half):
            block = reverse_bits(part * half + p, stages) ^ me
            place = reverse_bits((block // per_tp) ^ tp_me, tp_stages) * per_tp + block % per_tp
            sorted_ref[place] = product[p * rows : (p + 1) * rows]
    for p in range(half):
        keep_ref[p * rows : (p + 1) * rows, :] = sorted_ref[p].astype(bf16).astype(f32)
        send_ref[p * rows : (p + 1) * rows, :] = sorted_ref[half + p].astype(bf16)


def per_device(
    kv_size,
    tp_size,
    hidden_vectors,
    input_norm_gain,
    gate_matrix,
    value_matrix,
    write_matrix,
    read_matrix,
    step_matrix,
    raw_value_rows,
    raw_write_rows,
    raw_read_rows,
    value_filter_taps,
    write_filter_taps,
    read_filter_taps,
    step_size_bias,
    rate_logarithm,
    direct_path_gain,
    prior_step_preact,
    extra_log_decay,
    accepted,
    prior_state,
    group_norm_gain,
    output_matrix,
):
    stages = kv_size.bit_length() - 1
    tp_stages = tp_size.bit_length() - 1
    tokens, features = hidden_vectors.shape
    rows = tokens // kv_size
    seqs, heads, head_dim, width_n = prior_state.shape
    inner = heads * head_dim
    weights = (gate_matrix, value_matrix, write_matrix, read_matrix)
    width = sum(w.shape[1] for w in weights) + lanes
    swap = lambda x, axis, size, bit: lax.ppermute(x, axis, [(i, i ^ bit) for i in range(size)])
    line = lambda x: x.reshape(1, -1)
    shape = jax.ShapeDtypeStruct

    local = lambda x: pltpu.with_memory_space_constraint(x, pltpu.VMEM)
    near = lambda *x: pltpu.VMEM(*x)

    half = tokens // 2
    sources = (
        hidden_vectors.reshape(kv_size, rows, features),
        line(input_norm_gain),
        step_matrix.T,
        *weights,
    )
    keep, send = pl.pallas_call(
        functools.partial(project_body, stages),
        out_shape=(near((half, width), f32), near((half, width), bf16)),
        in_specs=[ANY] * len(sources),
        out_specs=(VMEM, VMEM),
        scratch_shapes=[pltpu.VMEM(x.shape, x.dtype) for x in sources]
        + [pltpu.VMEM((tokens, lanes), f32), pltpu.SemaphoreType.DMA((len(sources),))],
        compiler_params=PARAMS,
        name="project",
    )(*sources)

    groups = raw_write_rows.shape[2] // width_n
    columns = inner + 2 * groups * width_n
    taps, drafts = value_filter_taps.shape[0], prior_step_preact.shape[1]
    resumed, high, low, pre, small, gain = pl.pallas_call(
        resume_body,
        out_shape=(
            shape(prior_state.shape, f32),
            near((seqs, inner, width_n), bf16),
            near((seqs, inner, width_n), bf16),
            near((taps + 1, rows, columns), f32),
            near((4, rows, heads), f32),
            near((1, inner), f32),
        ),
        in_specs=[SMEM] + [VMEM] * 12 + [ANY],
        out_specs=(ANY,) + (VMEM,) * 5,
        scratch_shapes=[
            pltpu.VMEM(prior_state.shape, f32),
            pltpu.VMEM((seqs, raw_value_rows.shape[1] + 1, columns), f32),
            pltpu.VMEM((taps - 1 + drafts, columns), f32),
            pltpu.VMEM((taps, columns), f32),
            pltpu.VMEM((rows, inner + groups * width_n), f32),
            pltpu.SemaphoreType.DMA((seqs, groups)),
            pltpu.SemaphoreType.DMA((seqs, groups)),
        ],
        cost_estimate=pl.CostEstimate(flops=40_000_000, bytes_accessed=4_000_000, transcendentals=0),
        compiler_params=PARAMS,
        name="resume",
    )(
        accepted,
        raw_value_rows.transpose(1, 0, 2),
        raw_write_rows.transpose(1, 0, 2),
        raw_read_rows.transpose(1, 0, 2),
        value_filter_taps,
        write_filter_taps,
        read_filter_taps,
        line(step_size_bias),
        line(rate_logarithm),
        line(direct_path_gain),
        line(group_norm_gain),
        prior_step_preact,
        extra_log_decay,
        prior_state,
    )

    for stage in range(stages):
        recv = swap(send, "kv", kv_size, 1 << stage)
        if stage < stages - 1:
            half = half // 2
            keep, send = pl.pallas_call(
                combine_body,
                out_shape=(near((half, width), f32), near((half, width), bf16)),
                in_specs=[VMEM, VMEM, ANY],
                out_specs=(VMEM, VMEM),
                compiler_params=PARAMS,
                name="combine",
            )(local(keep), local(recv), local(small))

    normed = pl.pallas_call(
        functools.partial(mixer_body, features * kv_size),
        out_shape=near((rows, inner), bf16),
        in_specs=[VMEM] * 7,
        out_specs=VMEM,
        compiler_params=PARAMS,
        name="mixer",
    )(*(local(x) for x in (keep, recv, pre, small, high, low, gain)))

    for stage in reversed(range(stages)):
        recv = swap(normed, "kv", kv_size, 1 << stage)
        if stage > 0:
            normed = jnp.concatenate([normed, recv], axis=0)

    half = tokens // 2
    out_width = output_matrix.shape[1]
    keep, send = pl.pallas_call(
        functools.partial(output_body, stages, tp_stages),
        out_shape=(near((half, out_width), f32), near((half, out_width), bf16)),
        in_specs=[VMEM] * 3,
        out_specs=(VMEM, VMEM),
        scratch_shapes=[pltpu.VMEM((kv_size, rows, out_width), f32)],
        compiler_params=PARAMS,
        name="output",
    )(local(normed), local(recv), local(output_matrix))
    for stage in range(tp_stages):
        total = keep + swap(send, "tp", tp_size, 1 << stage).astype(f32)
        half = half // 2
        if stage < tp_stages - 1:
            keep, send = total[:half], total[half:]
    return total.astype(bf16), resumed


def solution(mesh):
    placed = (
        P(None, "kv"),
        P("kv"),
        P("kv", "tp"),
        P("kv", "tp"),
        P("kv", "tp"),
        P("kv", "tp"),
        P("kv", "tp"),
        P("kv", None, "tp"),
        P("kv", None, "tp"),
        P("kv", None, "tp"),
        P(None, "tp"),
        P(None, "tp"),
        P(None, "tp"),
        P("tp"),
        P("tp"),
        P("tp"),
        P("kv", None, "tp"),
        P("kv", None, "tp"),
        P("kv"),
        P("kv", "tp", None, None),
        P("tp"),
        P("tp", "kv"),
    )
    return jax.shard_map(
        functools.partial(per_device, mesh.shape["kv"], mesh.shape["tp"]),
        mesh=mesh,
        in_specs=placed,
        out_specs=(P("tp", "kv"), P("kv", "tp", None, None)),
        check_vma=False,
    )
```

```python
import functools

import jax
import jax.numpy as jnp
from jax import lax
from jax.experimental import pallas as pl
from jax.experimental.pallas import tpu as pltpu
from jax.sharding import PartitionSpec as P

epsilon = 1e-06
lanes = 128
half_lanes = lanes // 2
piece_bytes = 128 * 1024


VMEM = pl.BlockSpec(memory_space=pltpu.VMEM)
SMEM = pl.BlockSpec(memory_space=pltpu.SMEM)
ANY = pl.BlockSpec(memory_space=pl.ANY)
PARAMS = pltpu.CompilerParams(vmem_limit_bytes=24 * 2**20)
f32 = jnp.float32
bf16 = jnp.bfloat16


def reverse_bits(index, width):
    result = index * 0
    for bit in range(width):
        result = result | (((index >> bit) & 1) << (width - 1 - bit))
    return result


def split_pair(x):
    high = x.astype(bf16).astype(f32)
    return high, x - high


def fold_aux(aux):
    lane = lax.broadcasted_iota(jnp.int32, aux.shape, 1)
    return jnp.where(lane < half_lanes, aux + pltpu.roll(aux, half_lanes, 1), 0.0)


def pair_aux(aux):
    high, low = split_pair(aux)
    return (high + pltpu.roll(low, half_lanes, 1)).astype(bf16)


def silu(x):
    return x / (1.0 + jnp.exp(-x))


def softplus(x):
    return jnp.maximum(x, 0.0) + jnp.log1p(jnp.exp(-jnp.abs(x)))


def expander(heads, width):
    row = lax.broadcasted_iota(jnp.int32, (heads, width), 0)
    column = lax.broadcasted_iota(jnp.int32, (heads, width), 1)
    return (column // (width // heads) == row).astype(f32).astype(bf16)


def expand(x, matrix):
    rows = x.shape[0]
    high, low = split_pair(x)
    both = jnp.concatenate([high, low], axis=0).astype(bf16)
    wide = jnp.dot(both, matrix, preferred_element_type=f32)
    return wide[:rows] + wide[rows:]


def pieces(count, source, target):
    size = source.shape[0] // count
    return [(source.at[pl.ds(i * size, size)], target.at[pl.ds(i * size, size)]) for i in range(count)]


def project_body(stages, *refs):
    sources, (keep_ref, send_ref), buffers, (aux_ref, sems) = refs[:7], refs[7:9], refs[9:16], refs[16:]
    copies = []
    for source, buffer in zip(sources, buffers):
        parts = max(1, source.size * source.dtype.itemsize // piece_bytes)
        first = sum(len(c) for c in copies)
        copies.append(
            [
                pltpu.make_async_copy(src, dst, sems.at[first + i])
                for i, (src, dst) in enumerate(pieces(parts, source, buffer))
            ]
        )
        for copy in copies[-1]:
            copy.start()
    hidden_ref, gain_ref, step_ref = buffers[:3]
    me = lax.axis_index("kv")
    for copy in sum(copies[:3], []):
        copy.wait()
    blocks = [hidden_ref[reverse_bits(p, stages) ^ me] for p in range(1 << stages)]
    floats_in = jnp.concatenate([b.astype(f32) for b in blocks], axis=0)
    squares = jnp.sum(floats_in * floats_in, axis=1, keepdims=True)
    scaled = (floats_in * gain_ref[...]).astype(bf16)
    heads = step_ref.shape[0]
    half = floats_in.shape[0] // 2
    aux_ref[...] = jnp.zeros_like(aux_ref)
    aux_ref[:, :heads] = lax.dot_general(
        scaled, step_ref[...], (((1,), (1,)), ((), ())), preferred_element_type=f32
    )
    lane = lax.broadcasted_iota(jnp.int32, aux_ref.shape, 1)
    aux = jnp.where(lane == heads, squares, aux_ref[...])
    start = keep_ref.shape[1] - lanes
    keep_ref[:, start:] = aux[:half]
    send_ref[:, start:] = pair_aux(aux[half:])
    start = 0
    for copy, buffer in zip(copies[3:], buffers[3:]):
        for part in copy:
            part.wait()
        part = jnp.dot(scaled, buffer[...], preferred_element_type=f32)
        stop = start + buffer.shape[1]
        keep_ref[:, start:stop] = part[:half]
        send_ref[:, start:stop] = part[half:].astype(bf16)
        start = stop


def combine_body(keep_ref, recv_ref, _, next_ref, send_ref):
    half = next_ref.shape[0]
    start = keep_ref.shape[1] - lanes
    total = keep_ref[:, :start] + recv_ref[:, :start].astype(f32)
    next_ref[:, :start] = total[:half]
    send_ref[:, :start] = total[half:].astype(bf16)
    aux = fold_aux(keep_ref[:, start:] + recv_ref[:, start:].astype(f32))
    next_ref[:, start:] = aux[:half]
    send_ref[:, start:] = pair_aux(aux[half:])


def resume_body(
    accepted_ref,
    raw_value_ref,
    raw_write_ref,
    raw_read_ref,
    value_taps_ref,
    write_taps_ref,
    read_taps_ref,
    bias_ref,
    rate_ref,
    direct_ref,
    norm_gain_ref,
    prior_step_ref,
    extra_ref,
    state_in,
    state_out,
    high_ref,
    low_ref,
    pre_ref,
    small_ref,
    gain_ref,
    state_ref,
    raw_ref,
    window_ref,
    taps_ref,
    last_ref,
    in_sems,
    out_sems,
):
    seqs, heads, head_dim, width_n = state_ref.shape
    inner = heads * head_dim
    writes = raw_write_ref.shape[2]
    groups = writes // width_n
    per_group = heads // groups
    drafts = prior_step_ref.shape[1]
    taps = value_taps_ref.shape[0]
    places = [(s, g) for s in range(seqs) for g in range(groups)]

    def moving(s, g, source, target, sems):
        where = (s, pl.ds(g * per_group, per_group))
        return pltpu.make_async_copy(source.at[where], target.at[where], sems.at[s, g])

    for s, g in places:
        moving(s, g, state_in, state_ref, in_sems).start()
    cuts = (0, inner, inner + writes, inner + 2 * writes)
    roles = (
        (raw_value_ref, value_taps_ref),
        (raw_write_ref, write_taps_ref),
        (raw_read_ref, read_taps_ref),
    )
    for i, (_, tap_ref) in enumerate(roles):
        taps_ref[:, cuts[i] : cuts[i + 1]] = tap_ref[...].astype(f32)
    raw_rows = raw_value_ref.shape[0]
    raw_ref[...] = jnp.zeros_like(raw_ref)
    window_ref[...] = jnp.zeros_like(window_ref)
    for j in range(raw_rows):
        for i, (row_ref, _) in enumerate(roles):
            both = row_ref[j].astype(f32)
            for s in range(seqs):
                raw_ref[s, j : j + 1, cuts[i] : cuts[i + 1]] = both[s : s + 1]
    for s in range(seqs):
        count = accepted_ref[s]
        last = taps_ref[0:1, : cuts[2]] * raw_ref[s, 0:drafts, : cuts[2]]
        for j in range(1, taps):
            last = last + taps_ref[j : j + 1, : cuts[2]] * raw_ref[s, j : j + drafts, : cuts[2]]
        last_ref[s * drafts : (s + 1) * drafts, :] = silu(last)
        window = raw_ref[s, 0 : taps - 1, :]
        for a in range(1, drafts + 1):
            window = jnp.where(count == a, raw_ref[s, a : a + taps - 1, :], window)
        window_ref[: taps - 1, :] = window
        pre = taps_ref[0:1, :] * window_ref[0:drafts, :]
        for j in range(1, taps - 1):
            pre = pre + taps_ref[j : j + 1, :] * window_ref[j : j + drafts, :]
        pre_ref[0, s * drafts : (s + 1) * drafts, :] = pre
    rows = seqs * drafts
    wide_order = lax.broadcasted_iota(jnp.int32, (rows, cuts[3]), 0) % drafts
    for d in range(taps):
        pre_ref[d + 1] = jnp.where(wide_order >= d, taps_ref[taps - 1 - d : taps - d, :], 0.0)
    gain_ref[...] = norm_gain_ref[...]
    small_ref[0] = jnp.broadcast_to(bias_ref[...], (rows, heads))
    small_ref[1] = jnp.broadcast_to(jnp.exp(rate_ref[...]), (rows, heads))
    small_ref[2] = jnp.broadcast_to(direct_ref[...], (rows, heads))
    small_ref[3] = jnp.concatenate([extra_ref[s, drafts:] for s in range(seqs)], axis=0)
    row = lax.broadcasted_iota(jnp.int32, (rows, heads), 0)
    order = row % drafts
    count_of = jnp.full((rows, heads), accepted_ref[0], jnp.int32)
    for s in range(1, seqs):
        count_of = jnp.where(row >= s * drafts, accepted_ref[s], count_of)
    live = (order < count_of).astype(f32)
    preact = jnp.concatenate([prior_step_ref[s] for s in range(seqs)], axis=0)
    extra = jnp.concatenate([extra_ref[s, :drafts] for s in range(seqs)], axis=0)
    step = softplus(preact + bias_ref[...])
    kept = live * (extra - jnp.exp(rate_ref[...]) * step)
    tail = jnp.zeros_like(kept)
    for d in range(1, drafts):
        tail = tail + jnp.where(order + d < drafts, pltpu.roll(kept, rows - d, 0), 0.0)
    carry = jnp.exp(kept + tail)
    coefficient = expand(live * jnp.exp(tail) * step, expander(heads, inner))
    weighted = coefficient * last_ref[:, :inner]
    weighted_high, weighted_low = split_pair(weighted)
    write_high, write_low = split_pair(last_ref[:, inner:])
    wide_row = lax.broadcasted_iota(jnp.int32, (rows, inner), 0)
    right = jnp.concatenate([write_high, write_high, write_low, write_low], axis=0).astype(bf16)
    span = per_group * head_dim
    for s in range(seqs):
        own = (wide_row >= s * drafts) & (wide_row < (s + 1) * drafts)
        high = jnp.where(own, weighted_high, 0.0)
        low = jnp.where(own, weighted_low, 0.0)
        left = jnp.concatenate([high, low, high, low], axis=0).astype(bf16)
        for g in range(groups):
            added = lax.dot_general(
                left[:, g * span : (g + 1) * span],
                right[:, g * width_n : (g + 1) * width_n],
                (((0,), (0,)), ((), ())),
                preferred_element_type=f32,
            )
            moving(s, g, state_in, state_ref, in_sems).wait()
            for i in range(per_group):
                h = g * per_group + i
                factor = carry[s * drafts : s * drafts + 1, h : h + 1]
                fresh = factor * state_ref[s, h] + added[i * head_dim : (i + 1) * head_dim]
                state_ref[s, h] = fresh
                fresh_high, fresh_low = split_pair(fresh)
                high_ref[s, h * head_dim : (h + 1) * head_dim, :] = fresh_high.astype(bf16)
                low_ref[s, h * head_dim : (h + 1) * head_dim, :] = fresh_low.astype(bf16)
            moving(s, g, state_ref, state_out, out_sems).start()
    for s, g in places:
        moving(s, g, state_ref, state_out, out_sems).wait()


def mixer_body(
    features,
    keep_ref,
    recv_ref,
    pre_ref,
    small_ref,
    high_ref,
    low_ref,
    norm_gain_ref,
    out_ref,
):
    rows, inner = out_ref.shape
    heads = small_ref.shape[2]
    seqs, _, width_n = high_ref.shape
    drafts = rows // seqs
    taps = pre_ref.shape[0] - 1
    writes = (pre_ref.shape[2] - inner) // 2
    groups = writes // width_n
    span = inner // groups
    main = keep_ref.shape[1] - lanes
    order_of = lambda shape: lax.broadcasted_iota(jnp.int32, shape, 0) % drafts

    def back(x, d):
        if d == 0:
            return x
        return jnp.where(order_of(x.shape) >= d, pltpu.roll(x, d, 0), 0.0)

    aux = fold_aux(keep_ref[:, main:] + recv_ref[:, main:].astype(f32))
    inverse = lax.rsqrt(aux[:, heads : heads + 1] / features + epsilon)
    step_pre = aux[:, :heads] * inverse

    def role(start, stop):
        return inverse * (keep_ref[:, start:stop] + recv_ref[:, start:stop].astype(f32))

    def convolved(start, width):
        fresh = role(inner + start, inner + start + width)
        total = pre_ref[0, :, start : start + width]
        for d in range(taps):
            shifted = fresh if d == 0 else pltpu.roll(fresh, d, 0)
            total = total + pre_ref[d + 1, :, start : start + width] * shifted
        return silu(total)

    reads = convolved(inner + writes, writes)
    new_writes = convolved(inner, writes)

    step = softplus(step_pre + small_ref[0])
    log_decay = small_ref[3] - small_ref[1] * step
    total_decay = log_decay
    for d in range(1, drafts):
        total_decay = total_decay + back(log_decay, d)
    head = lax.broadcasted_iota(jnp.int32, (rows, heads), 1)
    small = [jnp.exp(total_decay)]
    for d in range(drafts):
        products = reads * back(new_writes, d)
        inner_term = jnp.zeros((rows, heads), f32)
        for g in range(groups):
            dot = jnp.sum(products[:, g * width_n : (g + 1) * width_n], axis=1, keepdims=True)
            inner_term = jnp.where(head // (heads // groups) == g, dot, inner_term)
        term = inner_term * back(step, d)
        if d == 0:
            term = term + small_ref[2]
        else:
            difference = jnp.minimum(total_decay - back(total_decay, d), 0.0)
            term = term * jnp.where(order_of(term.shape) >= d, jnp.exp(difference), 0.0)
        small.append(term)
    wide = expand(jnp.concatenate(small, axis=0), expander(heads, inner))

    reads_high, reads_low = split_pair(reads)
    reads_both = jnp.concatenate([reads_high, reads_low], axis=0).astype(bf16)
    across = (((1,), (1,)), ((), ()))
    values = convolved(0, inner)
    for g in range(groups):
        columns = slice(g * span, (g + 1) * span)
        left = reads_both[:, g * width_n : (g + 1) * width_n]
        carried = None
        for s in range(seqs):
            product = lax.dot_general(
                left, high_ref[s, columns, :], across, preferred_element_type=f32
            )
            fine = lax.dot_general(
                left[:rows], low_ref[s, columns, :], across, preferred_element_type=f32
            )
            product = product[:rows] + product[rows:] + fine
            if carried is None:
                carried = product
            else:
                row = lax.broadcasted_iota(jnp.int32, product.shape, 0)
                carried = jnp.where(row >= s * drafts, product, carried)
        mixed = carried * wide[:rows, columns]
        for d in range(drafts):
            mixed = mixed + wide[(d + 1) * rows : (d + 2) * rows, columns] * back(
                values[:, columns], d
            )
        gated = mixed * silu(role(g * span, (g + 1) * span))
        scale = lax.rsqrt(jnp.mean(gated * gated, axis=1, keepdims=True) + epsilon)
        out_ref[:, columns] = (gated * scale * norm_gain_ref[:, columns]).astype(bf16)


def output_body(stages, tp_stages, own_ref, recv_ref, weight_ref, keep_ref, send_ref, sorted_ref):
    me = lax.axis_index("kv")
    tp_me = lax.axis_index("tp")
    blocks = 1 << stages
    per_tp = blocks >> tp_stages
    rows = sorted_ref.shape[1]
    half = blocks // 2
    for part, ref in enumerate((own_ref, recv_ref)):
        product = jnp.dot(ref[...], weight_ref[...], preferred_element_type=f32)
        for p in range(half):
            block = reverse_bits(part * half + p, stages) ^ me
            place = reverse_bits((block // per_tp) ^ tp_me, tp_stages) * per_tp + block % per_tp
            sorted_ref[place] = product[p * rows : (p + 1) * rows]
    for p in range(half):
        keep_ref[p * rows : (p + 1) * rows, :] = sorted_ref[p].astype(bf16).astype(f32)
        send_ref[p * rows : (p + 1) * rows, :] = sorted_ref[half + p].astype(bf16)


def per_device(
    kv_size,
    tp_size,
    hidden_vectors,
    input_norm_gain,
    gate_matrix,
    value_matrix,
    write_matrix,
    read_matrix,
    step_matrix,
    raw_value_rows,
    raw_write_rows,
    raw_read_rows,
    value_filter_taps,
    write_filter_taps,
    read_filter_taps,
    step_size_bias,
    rate_logarithm,
    direct_path_gain,
    prior_step_preact,
    extra_log_decay,
    accepted,
    prior_state,
    group_norm_gain,
    output_matrix,
):
    stages = kv_size.bit_length() - 1
    tp_stages = tp_size.bit_length() - 1
    tokens, features = hidden_vectors.shape
    rows = tokens // kv_size
    seqs, heads, head_dim, width_n = prior_state.shape
    inner = heads * head_dim
    weights = (gate_matrix, value_matrix, write_matrix, read_matrix)
    width = sum(w.shape[1] for w in weights) + lanes
    swap = lambda x, axis, size, bit: lax.ppermute(x, axis, [(i, i ^ bit) for i in range(size)])
    line = lambda x: x.reshape(1, -1)
    shape = jax.ShapeDtypeStruct

    local = lambda x: pltpu.with_memory_space_constraint(x, pltpu.VMEM)
    far = lambda x: pltpu.with_memory_space_constraint(x, pltpu.HBM)
    near = lambda *x: pltpu.VMEM(*x)

    half = tokens // 2
    sources = (
        hidden_vectors.reshape(kv_size, rows, features),
        line(input_norm_gain),
        step_matrix.T,
        *weights,
    )
    keep, send = pl.pallas_call(
        functools.partial(project_body, stages),
        out_shape=(near((half, width), f32), near((half, width), bf16)),
        in_specs=[ANY] * len(sources),
        out_specs=(VMEM, VMEM),
        scratch_shapes=[pltpu.VMEM(x.shape, x.dtype) for x in sources]
        + [pltpu.VMEM((tokens, lanes), f32), pltpu.SemaphoreType.DMA((32,))],
        compiler_params=PARAMS,
        name="project",
    )(*(far(x) for x in sources))

    groups = raw_write_rows.shape[2] // width_n
    columns = inner + 2 * groups * width_n
    taps, drafts = value_filter_taps.shape[0], prior_step_preact.shape[1]
    resumed, high, low, pre, small, gain = pl.pallas_call(
        resume_body,
        out_shape=(
            shape(prior_state.shape, f32),
            near((seqs, inner, width_n), bf16),
            near((seqs, inner, width_n), bf16),
            near((taps + 1, rows, columns), f32),
            near((4, rows, heads), f32),
            near((1, inner), f32),
        ),
        in_specs=[SMEM] + [VMEM] * 12 + [ANY],
        out_specs=(ANY,) + (VMEM,) * 5,
        scratch_shapes=[
            pltpu.VMEM(prior_state.shape, f32),
            pltpu.VMEM((seqs, raw_value_rows.shape[1] + 1, columns), f32),
            pltpu.VMEM((taps - 1 + drafts, columns), f32),
            pltpu.VMEM((taps, columns), f32),
            pltpu.VMEM((rows, inner + groups * width_n), f32),
            pltpu.SemaphoreType.DMA((seqs, groups)),
            pltpu.SemaphoreType.DMA((seqs, groups)),
        ],
        cost_estimate=pl.CostEstimate(flops=40_000_000, bytes_accessed=4_000_000, transcendentals=0),
        compiler_params=PARAMS,
        name="resume",
    )(
        accepted,
        far(raw_value_rows.transpose(1, 0, 2)),
        far(raw_write_rows.transpose(1, 0, 2)),
        far(raw_read_rows.transpose(1, 0, 2)),
        far(value_filter_taps),
        far(write_filter_taps),
        far(read_filter_taps),
        far(line(step_size_bias)),
        far(line(rate_logarithm)),
        far(line(direct_path_gain)),
        far(line(group_norm_gain)),
        far(prior_step_preact),
        far(extra_log_decay),
        far(prior_state),
    )

    for stage in range(stages):
        recv = swap(send, "kv", kv_size, 1 << stage)
        if stage < stages - 1:
            half = half // 2
            keep, send = pl.pallas_call(
                combine_body,
                out_shape=(near((half, width), f32), near((half, width), bf16)),
                in_specs=[VMEM, VMEM, ANY],
                out_specs=(VMEM, VMEM),
                compiler_params=PARAMS,
                name="combine",
            )(local(keep), local(recv), local(small))

    normed = pl.pallas_call(
        functools.partial(mixer_body, features * kv_size),
        out_shape=near((rows, inner), bf16),
        in_specs=[VMEM] * 7,
        out_specs=VMEM,
        compiler_params=PARAMS,
        name="mixer",
    )(*(local(x) for x in (keep, recv, pre, small, high, low, gain)))

    for stage in reversed(range(stages)):
        recv = swap(normed, "kv", kv_size, 1 << stage)
        if stage > 0:
            normed = jnp.concatenate([normed, recv], axis=0)

    half = tokens // 2
    out_width = output_matrix.shape[1]
    keep, send = pl.pallas_call(
        functools.partial(output_body, stages, tp_stages),
        out_shape=(near((half, out_width), f32), near((half, out_width), bf16)),
        in_specs=[VMEM] * 3,
        out_specs=(VMEM, VMEM),
        scratch_shapes=[pltpu.VMEM((kv_size, rows, out_width), f32)],
        compiler_params=PARAMS,
        name="output",
    )(local(normed), local(recv), local(output_matrix))
    for stage in range(tp_stages):
        total = keep + swap(send, "tp", tp_size, 1 << stage).astype(f32)
        half = half // 2
        if stage < tp_stages - 1:
            keep, send = total[:half], total[half:]
    return total.astype(bf16), resumed


def solution(mesh):
    placed = (
        P(None, "kv"),
        P("kv"),
        P("kv", "tp"),
        P("kv", "tp"),
        P("kv", "tp"),
        P("kv", "tp"),
        P("kv", "tp"),
        P("kv", None, "tp"),
        P("kv", None, "tp"),
        P("kv", None, "tp"),
        P(None, "tp"),
        P(None, "tp"),
        P(None, "tp"),
        P("tp"),
        P("tp"),
        P("tp"),
        P("kv", None, "tp"),
        P("kv", None, "tp"),
        P("kv"),
        P("kv", "tp", None, None),
        P("tp"),
        P("tp", "kv"),
    )
    return jax.shard_map(
        functools.partial(per_device, mesh.shape["kv"], mesh.shape["tp"]),
        mesh=mesh,
        in_specs=placed,
        out_specs=(P("tp", "kv"), P("kv", "tp", None, None)),
        check_vma=False,
    )
```

```python
import functools

import jax
import jax.numpy as jnp
from jax import lax
from jax.experimental import pallas as pl
from jax.experimental.pallas import tpu as pltpu
from jax.sharding import PartitionSpec as P

epsilon = 1e-06
lanes = 128
half_lanes = lanes // 2
piece_bytes = 128 * 1024


VMEM = pl.BlockSpec(memory_space=pltpu.VMEM)
SMEM = pl.BlockSpec(memory_space=pltpu.SMEM)
ANY = pl.BlockSpec(memory_space=pl.ANY)
PARAMS = pltpu.CompilerParams(vmem_limit_bytes=24 * 2**20)
f32 = jnp.float32
bf16 = jnp.bfloat16


def reverse_bits(index, width):
    result = index * 0
    for bit in range(width):
        result = result | (((index >> bit) & 1) << (width - 1 - bit))
    return result


def direct_bits(stages):
    return min(2, stages - 1)


def partners(bits):
    return {0: (), 1: (1,), 2: (1, 3, 2)}[bits]


def parity(index, width):
    result = index & 1
    for bit in range(1, width):
        result = result ^ ((index >> bit) & 1)
    return result


def split_pair(x):
    high = x.astype(bf16).astype(f32)
    return high, x - high


def fold_aux(aux):
    lane = lax.broadcasted_iota(jnp.int32, aux.shape, 1)
    return jnp.where(lane < half_lanes, aux + pltpu.roll(aux, half_lanes, 1), 0.0)


def pair_aux(aux):
    high, low = split_pair(aux)
    return (high + pltpu.roll(low, half_lanes, 1)).astype(bf16)


def silu(x):
    return x / (1.0 + jnp.exp(-x))


def softplus(x):
    return jnp.maximum(x, 0.0) + jnp.log1p(jnp.exp(-jnp.abs(x)))


def expander(heads, width):
    row = lax.broadcasted_iota(jnp.int32, (heads, width), 0)
    column = lax.broadcasted_iota(jnp.int32, (heads, width), 1)
    return (column // (width // heads) == row).astype(f32).astype(bf16)


def expand(x, matrix):
    rows = x.shape[0]
    high, low = split_pair(x)
    both = jnp.concatenate([high, low], axis=0).astype(bf16)
    wide = jnp.dot(both, matrix, preferred_element_type=f32)
    return wide[:rows] + wide[rows:]


def pieces(count, source, target):
    size = source.shape[0] // count
    return [(source.at[pl.ds(i * size, size)], target.at[pl.ds(i * size, size)]) for i in range(count)]


def project_body(stages, *refs):
    bits = direct_bits(stages)
    parts = 1 << bits
    sources, (keep_ref, *send_refs), refs = refs[:7], refs[7 : 7 + parts], refs[7 + parts :]
    buffers, (aux_ref, sems) = refs[:7], refs[7:]
    copies = []
    for source, buffer in zip(sources, buffers):
        count = max(1, source.size * source.dtype.itemsize // piece_bytes)
        first = sum(len(c) for c in copies)
        copies.append(
            [
                pltpu.make_async_copy(src, dst, sems.at[first + i])
                for i, (src, dst) in enumerate(pieces(count, source, buffer))
            ]
        )
        for copy in copies[-1]:
            copy.start()
    hidden_ref, gain_ref, step_ref = buffers[:3]
    me = lax.axis_index("kv")
    for copy in sum(copies[:3], []):
        copy.wait()
    blocks = [hidden_ref[reverse_bits(p, stages) ^ me] for p in range(1 << stages)]
    floats_in = jnp.concatenate([b.astype(f32) for b in blocks], axis=0)
    squares = jnp.sum(floats_in * floats_in, axis=1, keepdims=True)
    scaled = (floats_in * gain_ref[...]).astype(bf16)
    heads = step_ref.shape[0]
    share = keep_ref.shape[0]
    places = [reverse_bits(partner, bits) * share for partner in partners(bits)]
    aux_ref[...] = jnp.zeros_like(aux_ref)
    aux_ref[:, :heads] = lax.dot_general(
        scaled, step_ref[...], (((1,), (1,)), ((), ())), preferred_element_type=f32
    )
    lane = lax.broadcasted_iota(jnp.int32, aux_ref.shape, 1)
    aux = jnp.where(lane == heads, squares, aux_ref[...])
    start = keep_ref.shape[1] - lanes
    keep_ref[:, start:] = aux[:share]
    for place, send_ref in zip(places, send_refs):
        send_ref[:, start:] = pair_aux(aux[place : place + share])
    start = 0
    for copy, buffer in zip(copies[3:], buffers[3:]):
        for part in copy:
            part.wait()
        part = jnp.dot(scaled, buffer[...], preferred_element_type=f32)
        stop = start + buffer.shape[1]
        keep_ref[:, start:stop] = part[:share]
        for place, send_ref in zip(places, send_refs):
            send_ref[:, start:stop] = part[place : place + share].astype(bf16)
        start = stop


def combine_body(keep_ref, *refs):
    *recv_refs, _, next_ref, send_ref = refs
    half = next_ref.shape[0]
    start = keep_ref.shape[1] - lanes
    total = keep_ref[:, :start]
    aux = keep_ref[:, start:]
    for recv_ref in recv_refs:
        total = total + recv_ref[:, :start].astype(f32)
        aux = aux + recv_ref[:, start:].astype(f32)
    next_ref[:, :start] = total[:half]
    send_ref[:, :start] = total[half:].astype(bf16)
    aux = fold_aux(aux)
    next_ref[:, start:] = aux[:half]
    send_ref[:, start:] = pair_aux(aux[half:])


def resume_body(
    accepted_ref,
    raw_value_ref,
    raw_write_ref,
    raw_read_ref,
    value_taps_ref,
    write_taps_ref,
    read_taps_ref,
    bias_ref,
    rate_ref,
    direct_ref,
    norm_gain_ref,
    prior_step_ref,
    extra_ref,
    state_in,
    _,
    state_out,
    high_ref,
    low_ref,
    pre_ref,
    small_ref,
    gain_ref,
    state_ref,
    raw_ref,
    window_ref,
    taps_ref,
    last_ref,
    in_sems,
    out_sems,
):
    seqs, heads, head_dim, width_n = state_ref.shape
    inner = heads * head_dim
    writes = raw_write_ref.shape[2]
    groups = writes // width_n
    per_group = heads // groups
    drafts = prior_step_ref.shape[1]
    taps = value_taps_ref.shape[0]
    places = [(s, g) for s in range(seqs) for g in range(groups)]

    def moving(s, g, source, target, sems):
        where = (s, pl.ds(g * per_group, per_group))
        return pltpu.make_async_copy(source.at[where], target.at[where], sems.at[s, g])

    for s, g in places:
        moving(s, g, state_in, state_ref, in_sems).start()
    cuts = (0, inner, inner + writes, inner + 2 * writes)
    roles = (
        (raw_value_ref, value_taps_ref),
        (raw_write_ref, write_taps_ref),
        (raw_read_ref, read_taps_ref),
    )
    for i, (_, tap_ref) in enumerate(roles):
        taps_ref[:, cuts[i] : cuts[i + 1]] = tap_ref[...].astype(f32)
    raw_rows = raw_value_ref.shape[0]
    raw_ref[...] = jnp.zeros_like(raw_ref)
    window_ref[...] = jnp.zeros_like(window_ref)
    for j in range(raw_rows):
        for i, (row_ref, _) in enumerate(roles):
            both = row_ref[j].astype(f32)
            for s in range(seqs):
                raw_ref[s, j : j + 1, cuts[i] : cuts[i + 1]] = both[s : s + 1]
    for s in range(seqs):
        count = accepted_ref[s]
        last = taps_ref[0:1, : cuts[2]] * raw_ref[s, 0:drafts, : cuts[2]]
        for j in range(1, taps):
            last = last + taps_ref[j : j + 1, : cuts[2]] * raw_ref[s, j : j + drafts, : cuts[2]]
        last_ref[s * drafts : (s + 1) * drafts, :] = silu(last)
        window = raw_ref[s, 0 : taps - 1, :]
        for a in range(1, drafts + 1):
            window = jnp.where(count == a, raw_ref[s, a : a + taps - 1, :], window)
        window_ref[: taps - 1, :] = window
        pre = taps_ref[0:1, :] * window_ref[0:drafts, :]
        for j in range(1, taps - 1):
            pre = pre + taps_ref[j : j + 1, :] * window_ref[j : j + drafts, :]
        pre_ref[0, s * drafts : (s + 1) * drafts, :] = pre
    rows = seqs * drafts
    wide_order = lax.broadcasted_iota(jnp.int32, (rows, cuts[3]), 0) % drafts
    for d in range(taps):
        pre_ref[d + 1] = jnp.where(wide_order >= d, taps_ref[taps - 1 - d : taps - d, :], 0.0)
    gain_ref[...] = norm_gain_ref[...]
    small_ref[0] = jnp.broadcast_to(bias_ref[...], (rows, heads))
    small_ref[1] = jnp.broadcast_to(jnp.exp(rate_ref[...]), (rows, heads))
    small_ref[2] = jnp.broadcast_to(direct_ref[...], (rows, heads))
    small_ref[3] = jnp.concatenate([extra_ref[s, drafts:] for s in range(seqs)], axis=0)
    row = lax.broadcasted_iota(jnp.int32, (rows, heads), 0)
    order = row % drafts
    count_of = jnp.full((rows, heads), accepted_ref[0], jnp.int32)
    for s in range(1, seqs):
        count_of = jnp.where(row >= s * drafts, accepted_ref[s], count_of)
    live = (order < count_of).astype(f32)
    preact = jnp.concatenate([prior_step_ref[s] for s in range(seqs)], axis=0)
    extra = jnp.concatenate([extra_ref[s, :drafts] for s in range(seqs)], axis=0)
    step = softplus(preact + bias_ref[...])
    kept = live * (extra - jnp.exp(rate_ref[...]) * step)
    tail = jnp.zeros_like(kept)
    for d in range(1, drafts):
        tail = tail + jnp.where(order + d < drafts, pltpu.roll(kept, rows - d, 0), 0.0)
    carry = jnp.exp(kept + tail)
    coefficient = expand(live * jnp.exp(tail) * step, expander(heads, inner))
    weighted = coefficient * last_ref[:, :inner]
    weighted_high, weighted_low = split_pair(weighted)
    write_high, write_low = split_pair(last_ref[:, inner:])
    wide_row = lax.broadcasted_iota(jnp.int32, (rows, inner), 0)
    right = jnp.concatenate([write_high, write_high, write_low, write_low], axis=0).astype(bf16)
    span = per_group * head_dim
    for s in range(seqs):
        own = (wide_row >= s * drafts) & (wide_row < (s + 1) * drafts)
        high = jnp.where(own, weighted_high, 0.0)
        low = jnp.where(own, weighted_low, 0.0)
        left = jnp.concatenate([high, low, high, low], axis=0).astype(bf16)
        for g in range(groups):
            added = lax.dot_general(
                left[:, g * span : (g + 1) * span],
                right[:, g * width_n : (g + 1) * width_n],
                (((0,), (0,)), ((), ())),
                preferred_element_type=f32,
            )
            moving(s, g, state_in, state_ref, in_sems).wait()
            for i in range(per_group):
                h = g * per_group + i
                factor = carry[s * drafts : s * drafts + 1, h : h + 1]
                fresh = factor * state_ref[s, h] + added[i * head_dim : (i + 1) * head_dim]
                state_ref[s, h] = fresh
                fresh_high, fresh_low = split_pair(fresh)
                high_ref[s, h * head_dim : (h + 1) * head_dim, :] = fresh_high.astype(bf16)
                low_ref[s, h * head_dim : (h + 1) * head_dim, :] = fresh_low.astype(bf16)
            moving(s, g, state_ref, state_out, out_sems).start()
    for s, g in places:
        moving(s, g, state_ref, state_out, out_sems).wait()


def mixer_body(
    features,
    keep_ref,
    recv_ref,
    pre_ref,
    small_ref,
    high_ref,
    low_ref,
    norm_gain_ref,
    out_ref,
):
    rows, inner = out_ref.shape
    heads = small_ref.shape[2]
    seqs, _, width_n = high_ref.shape
    drafts = rows // seqs
    taps = pre_ref.shape[0] - 1
    writes = (pre_ref.shape[2] - inner) // 2
    groups = writes // width_n
    span = inner // groups
    main = keep_ref.shape[1] - lanes
    order_of = lambda shape: lax.broadcasted_iota(jnp.int32, shape, 0) % drafts

    def back(x, d):
        if d == 0:
            return x
        return jnp.where(order_of(x.shape) >= d, pltpu.roll(x, d, 0), 0.0)

    aux = fold_aux(keep_ref[:, main:] + recv_ref[:, main:].astype(f32))
    inverse = lax.rsqrt(aux[:, heads : heads + 1] / features + epsilon)
    step_pre = aux[:, :heads] * inverse

    def role(start, stop):
        return inverse * (keep_ref[:, start:stop] + recv_ref[:, start:stop].astype(f32))

    def convolved(start, width):
        fresh = role(inner + start, inner + start + width)
        total = pre_ref[0, :, start : start + width]
        for d in range(taps):
            shifted = fresh if d == 0 else pltpu.roll(fresh, d, 0)
            total = total + pre_ref[d + 1, :, start : start + width] * shifted
        return silu(total)

    reads = convolved(inner + writes, writes)
    new_writes = convolved(inner, writes)

    step = softplus(step_pre + small_ref[0])
    log_decay = small_ref[3] - small_ref[1] * step
    total_decay = log_decay
    for d in range(1, drafts):
        total_decay = total_decay + back(log_decay, d)
    head = lax.broadcasted_iota(jnp.int32, (rows, heads), 1)
    small = [jnp.exp(total_decay)]
    for d in range(drafts):
        products = reads * back(new_writes, d)
        inner_term = jnp.zeros((rows, heads), f32)
        for g in range(groups):
            dot = jnp.sum(products[:, g * width_n : (g + 1) * width_n], axis=1, keepdims=True)
            inner_term = jnp.where(head // (heads // groups) == g, dot, inner_term)
        term = inner_term * back(step, d)
        if d == 0:
            term = term + small_ref[2]
        else:
            difference = jnp.minimum(total_decay - back(total_decay, d), 0.0)
            term = term * jnp.where(order_of(term.shape) >= d, jnp.exp(difference), 0.0)
        small.append(term)
    wide = expand(jnp.concatenate(small, axis=0), expander(heads, inner))

    reads_high, reads_low = split_pair(reads)
    reads_both = jnp.concatenate([reads_high, reads_low], axis=0).astype(bf16)
    across = (((1,), (1,)), ((), ()))
    values = convolved(0, inner)
    for g in range(groups):
        columns = slice(g * span, (g + 1) * span)
        left = reads_both[:, g * width_n : (g + 1) * width_n]
        carried = None
        for s in range(seqs):
            product = lax.dot_general(
                left, high_ref[s, columns, :], across, preferred_element_type=f32
            )
            fine = lax.dot_general(
                left[:rows], low_ref[s, columns, :], across, preferred_element_type=f32
            )
            product = product[:rows] + product[rows:] + fine
            if carried is None:
                carried = product
            else:
                row = lax.broadcasted_iota(jnp.int32, product.shape, 0)
                carried = jnp.where(row >= s * drafts, product, carried)
        mixed = carried * wide[:rows, columns]
        for d in range(drafts):
            mixed = mixed + wide[(d + 1) * rows : (d + 2) * rows, columns] * back(
                values[:, columns], d
            )
        gated = mixed * silu(role(g * span, (g + 1) * span))
        scale = lax.rsqrt(jnp.mean(gated * gated, axis=1, keepdims=True) + epsilon)
        out_ref[:, columns] = (gated * scale * norm_gain_ref[:, columns]).astype(bf16)


def output_body(held, tp_stages, per_tp, *refs):
    operands, refs = refs[: len(held)], refs[len(held) :]
    *weights, keep_ref, send_ref, sorted_ref = refs
    me = lax.axis_index("kv")
    tp_me = lax.axis_index("tp")
    blocks, rows, _ = sorted_ref.shape
    for whose, weight_ref in enumerate(weights):
        mine = [
            (offset, ref[i * rows : (i + 1) * rows])
            for ref, names in zip(operands, held)
            for i, (offset, owner) in enumerate(names)
            if owner == whose
        ]
        left = jnp.concatenate([x for _, x in mine], axis=0)
        product = jnp.dot(left, weight_ref[...], preferred_element_type=f32)
        for i, (offset, _) in enumerate(mine):
            block = me ^ offset
            target = (block // per_tp) ^ tp_me
            target = (target & ~1) | parity(target, tp_stages)
            place = reverse_bits(target, tp_stages) * per_tp + block % per_tp
            sorted_ref[place] = product[i * rows : (i + 1) * rows]
    half = blocks // 2
    for p in range(half):
        keep_ref[p * rows : (p + 1) * rows, :] = sorted_ref[p].astype(bf16).astype(f32)
        send_ref[p * rows : (p + 1) * rows, :] = sorted_ref[half + p].astype(bf16)


def per_device(
    kv_size,
    tp_size,
    hidden_vectors,
    input_norm_gain,
    gate_matrix,
    value_matrix,
    write_matrix,
    read_matrix,
    step_matrix,
    raw_value_rows,
    raw_write_rows,
    raw_read_rows,
    value_filter_taps,
    write_filter_taps,
    read_filter_taps,
    step_size_bias,
    rate_logarithm,
    direct_path_gain,
    prior_step_preact,
    extra_log_decay,
    accepted,
    prior_state,
    group_norm_gain,
    output_matrix,
):
    stages = kv_size.bit_length() - 1
    tp_stages = tp_size.bit_length() - 1
    tokens, features = hidden_vectors.shape
    rows = tokens // kv_size
    seqs, heads, head_dim, width_n = prior_state.shape
    inner = heads * head_dim
    weights = (gate_matrix, value_matrix, write_matrix, read_matrix)
    width = sum(w.shape[1] for w in weights) + lanes
    bits = direct_bits(stages)
    cross = 1 if tp_size > 1 else 0

    def swap(x, kv_offset, tp_offset):
        pairs = [
            (k * tp_size + t, (k ^ kv_offset) * tp_size + (t ^ tp_offset))
            for k in range(kv_size)
            for t in range(tp_size)
        ]
        return lax.ppermute(x, ("kv", "tp"), pairs)

    line = lambda x: x.reshape(1, -1)
    shape = jax.ShapeDtypeStruct

    local = lambda x: pltpu.with_memory_space_constraint(x, pltpu.VMEM)
    far = lambda x: pltpu.with_memory_space_constraint(x, pltpu.HBM)
    near = lambda *x: pltpu.VMEM(*x)

    share = tokens >> bits
    sources = (
        hidden_vectors.reshape(kv_size, rows, features),
        line(input_norm_gain),
        step_matrix.T,
        *weights,
    )
    keep, *sends = pl.pallas_call(
        functools.partial(project_body, stages),
        out_shape=(near((share, width), f32),) + (near((share, width), bf16),) * ((1 << bits) - 1),
        in_specs=[ANY] * len(sources),
        out_specs=(VMEM,) * (1 << bits),
        scratch_shapes=[pltpu.VMEM(x.shape, x.dtype) for x in sources]
        + [pltpu.VMEM((tokens, lanes), f32), pltpu.SemaphoreType.DMA((32,))],
        compiler_params=PARAMS,
        name="project",
    )(*(far(x) for x in sources))

    groups = raw_write_rows.shape[2] // width_n
    columns = inner + 2 * groups * width_n
    taps, drafts = value_filter_taps.shape[0], prior_step_preact.shape[1]
    resumed, high, low, pre, small, gain = pl.pallas_call(
        resume_body,
        out_shape=(
            shape(prior_state.shape, f32),
            near((seqs, inner, width_n), bf16),
            near((seqs, inner, width_n), bf16),
            near((taps + 1, rows, columns), f32),
            near((4, rows, heads), f32),
            near((1, inner), f32),
        ),
        in_specs=[SMEM] + [VMEM] * 12 + [ANY] * 2,
        out_specs=(ANY,) + (VMEM,) * 5,
        scratch_shapes=[
            pltpu.VMEM(prior_state.shape, f32),
            pltpu.VMEM((seqs, raw_value_rows.shape[1] + 1, columns), f32),
            pltpu.VMEM((taps - 1 + drafts, columns), f32),
            pltpu.VMEM((taps, columns), f32),
            pltpu.VMEM((rows, inner + groups * width_n), f32),
            pltpu.SemaphoreType.DMA((seqs, groups)),
            pltpu.SemaphoreType.DMA((seqs, groups)),
        ],
        cost_estimate=pl.CostEstimate(flops=40_000_000, bytes_accessed=4_000_000, transcendentals=0),
        compiler_params=PARAMS,
        name="resume",
    )(
        far(accepted),
        far(raw_value_rows.transpose(1, 0, 2)),
        far(raw_write_rows.transpose(1, 0, 2)),
        far(raw_read_rows.transpose(1, 0, 2)),
        far(value_filter_taps),
        far(write_filter_taps),
        far(read_filter_taps),
        far(line(step_size_bias)),
        far(line(rate_logarithm)),
        far(line(direct_path_gain)),
        far(line(group_norm_gain)),
        far(prior_step_preact),
        far(extra_log_decay),
        far(prior_state),
        local(keep),
    )

    recvs = [swap(send, partner, 0) for partner, send in zip(partners(bits), sends)]
    for stage in range(bits, stages):
        share = share // 2
        keep, send = pl.pallas_call(
            combine_body,
            out_shape=(near((share, width), f32), near((share, width), bf16)),
            in_specs=[VMEM] * (1 + len(recvs)) + [ANY],
            out_specs=(VMEM, VMEM),
            compiler_params=PARAMS,
            name="combine",
        )(*(local(x) for x in (keep, *recvs, small)))
        recvs = [swap(send, 1 << stage, 0)]
    recv = recvs[0]

    normed = pl.pallas_call(
        functools.partial(mixer_body, features * kv_size),
        out_shape=near((rows, inner), bf16),
        in_specs=[VMEM] * 7,
        out_specs=VMEM,
        compiler_params=PARAMS,
        name="mixer",
    )(*(local(x) for x in (keep, recv, pre, small, high, low, gain)))

    weights_out = [output_matrix]
    if cross:
        weights_out.append(swap(lax.optimization_barrier((output_matrix, keep))[0], 0, 1))
    names = [(0, 0)]
    for stage in reversed(range(bits, stages)):
        recv = swap(normed, 1 << stage, cross)
        normed = jnp.concatenate([normed, recv], axis=0)
        names = names + [(offset ^ (1 << stage), owner ^ cross) for offset, owner in names]
    operands, held = [normed], [tuple(names)]
    for partner in reversed(partners(bits)):
        operands.append(swap(normed, partner, cross))
        held.append(tuple((offset ^ partner, owner ^ cross) for offset, owner in names))

    half = tokens // 2
    out_width = output_matrix.shape[1]
    keep, send = pl.pallas_call(
        functools.partial(output_body, tuple(held), tp_stages, kv_size // tp_size),
        out_shape=(near((half, out_width), f32), near((half, out_width), bf16)),
        in_specs=[VMEM] * (len(operands) + len(weights_out)),
        out_specs=(VMEM, VMEM),
        scratch_shapes=[pltpu.VMEM((kv_size, rows, out_width), f32)],
        compiler_params=PARAMS,
        name="output",
    )(*(local(x) for x in (*operands, *weights_out)))
    for stage in range(tp_stages):
        total = keep + swap(send, 0, (1 << stage) | 1).astype(f32)
        half = half // 2
        if stage < tp_stages - 1:
            keep, send = total[:half], total[half:]
    return total.astype(bf16), resumed


def solution(mesh):
    placed = (
        P(None, "kv"),
        P("kv"),
        P("kv", "tp"),
        P("kv", "tp"),
        P("kv", "tp"),
        P("kv", "tp"),
        P("kv", "tp"),
        P("kv", None, "tp"),
        P("kv", None, "tp"),
        P("kv", None, "tp"),
        P(None, "tp"),
        P(None, "tp"),
        P(None, "tp"),
        P("tp"),
        P("tp"),
        P("tp"),
        P("kv", None, "tp"),
        P("kv", None, "tp"),
        P("kv"),
        P("kv", "tp", None, None),
        P("tp"),
        P("tp", "kv"),
    )
    return jax.shard_map(
        functools.partial(per_device, mesh.shape["kv"], mesh.shape["tp"]),
        mesh=mesh,
        in_specs=placed,
        out_specs=(P("tp", "kv"), P("kv", "tp", None, None)),
        check_vma=False,
    )
```
